32 devices in a mesh: sp: 8 (over z, y), tp: 4 (over x, core).
Axes of the slice: x: 2, y: 2, z: 4, core: 2. Of those that a mesh axis runs over, the one named last changes fastest.
Arguments:
- tokens: bfloat16 [2048, 2048], P(('sp', 'tp')), may hold values from -6 to 6
- norm_gain: float32 [2048], replicated, may hold values from 0.1 to 1.9
- query_weight: bfloat16 [1024, 2048], P('tp', 'sp'), may hold values from -0.088609319 to 0.088609319
- key_weight: bfloat16 [256, 2048], P('tp', 'sp'), may hold values from -0.10628699 to 0.10628699
- value_weight: bfloat16 [256, 2048], P('tp', 'sp'), may hold values from -0.125 to 0.125
- gate_weight: bfloat16 [1024, 2048], P('tp', 'sp'), may hold values from -0.125 to 0.125
- left_weight: bfloat16 [1024, 2048], P('tp', 'sp'), may hold values from -0.125 to 0.125
- input_weight: bfloat16 [1024, 2048], P('tp', 'sp'), may hold values from -0.125 to 0.125
- query_gain: float32 [64], replicated, may hold values from 0.3 to 4.5, as said below
- key_gain: float32 [64], replicated, may hold values from 0.3 to 4.5, as said below
- sink_logit: float32 [16], P('tp'), may hold values from 2 to 7
- conv_weight: float32 [3, 1024], P(None, 'tp'), may hold values from -3 to 3
- out_attention: bfloat16 [1024, 2048], P('tp', 'sp'), may hold values from -0.125 to 0.125
- out_conv: bfloat16 [1024, 2048], P('tp', 'sp'), may hold values from -0.125 to 0.125
Outputs:
- mixed: bfloat16 [2048, 2048], P(('sp', 'tp'))
The draws below stay inside these ranges and needn't reach their ends.
Inputs may be any that keep to these rules, and one draw needn't show every extreme that they name: `query_gain`: positive. `key_gain`: positive.
All inputs are finite; a program needn't handle non-finite values.
Results may differ from the reference program's by a relative error of at most 0.024.
Values may be sent and summed in bfloat16 or wider, within the bound.
A program may use at most 64 MiB of HBM per device.

```python
import jax
import jax.numpy as jnp
from jax import lax

D = 2048
HEAD_DIM = 64
Q_HEADS = 16
KV_HEADS = 4
CONV_CH = 1024
WINDOW = 128
BLOCK = 128
TOKENS = 2048
N_TP = 4


def shared_query(key):
    return jnp.clip(jax.random.normal(jax.random.fold_in(key, 101), (Q_HEADS * HEAD_DIM, D), jnp.float32), -4.0, 4.0) * D ** (-0.5)


def draw_query_weight(key, part):
    return shared_query(key).astype(jnp.bfloat16)


def draw_key_weight(key, part):
    noise = jnp.clip(jax.random.normal(jax.random.fold_in(key, 102), (KV_HEADS * HEAD_DIM, D), jnp.float32), -4.0, 4.0) * D ** (-0.5)
    result = noise
    return result.astype(jnp.bfloat16)


def draw_query_gain(key, part):
    result = jax.random.uniform(jax.random.fold_in(key, 103), (HEAD_DIM,), jnp.float32, 0.3, 1.9)
    return result


def draw_key_gain(key, part):
    result = jax.random.uniform(jax.random.fold_in(key, 104), (HEAD_DIM,), jnp.float32, 0.3, 1.9)
    return result


def level_of(rng, shape, cuts, least, top_value):
    def one(axis_at, parts):
        draws = jax.random.uniform(jax.random.fold_in(jax.random.fold_in(rng, 6), axis_at), (parts,), jnp.float32, least / len(cuts), top_value / len(cuts))
        return jnp.repeat(jnp.exp(draws), shape[axis_at] // parts).reshape((-1,) + (1,) * (len(shape) - axis_at - 1))

    loudness = one(*cuts[0])
    for cut in cuts[1:]:
        loudness = loudness * one(*cut)
    return loudness


def centred(own_key, extent, deviation, limit, split=(), held_as=jnp.bfloat16):
    level = level_of(own_key, extent, split, -0.22, 0.18) if split else 1.0
    drawn = jax.random.normal(own_key, extent, jnp.float32) * deviation * level
    return jnp.minimum(jnp.maximum(drawn, -limit), limit).astype(held_as)


def setup_inputs(seed: int = 0) -> dict:
    splits = jax.random.split(jax.random.key(seed), 15)
    return {
        "tokens": centred(splits[0], (TOKENS, D), 1.0, 6.0, ((0, 32),)),
        "norm_gain": jnp.clip(1.0 + 0.18 * jax.random.normal(splits[1], (D,), jnp.float32), 0.1, 1.9),
        "query_weight": draw_query_weight(jax.random.fold_in(splits[14], 71), 0),
        "key_weight": draw_key_weight(jax.random.fold_in(splits[14], 71), 0),
        "value_weight": centred(splits[4], (KV_HEADS * HEAD_DIM, D), D ** -0.5, 0.125, ((0, 4), (1, 8))),
        "gate_weight": centred(splits[5], (CONV_CH, D), D ** -0.5, 0.125, ((0, 4), (1, 8))),
        "left_weight": centred(splits[6], (CONV_CH, D), D ** -0.5, 0.125, ((0, 4), (1, 8))),
        "input_weight": centred(splits[7], (CONV_CH, D), D ** -0.5, 0.125, ((0, 4), (1, 8))),
        "query_gain": draw_query_gain(jax.random.fold_in(splits[14], 71), 0),
        "key_gain": draw_key_gain(jax.random.fold_in(splits[14], 71), 0),
        "sink_logit": jnp.clip(2.0 + 5.0 * jax.random.uniform(splits[10], (Q_HEADS,), jnp.float32) ** level_of(splits[10], (Q_HEADS,), ((0, 4),), -0.2, 0.2), 2.0, 7.0),
        "conv_weight": centred(splits[11], (3, CONV_CH), 0.6, 3.0, ((1, 4),), jnp.float32),
        "out_attention": centred(splits[12], (Q_HEADS * HEAD_DIM, D), (Q_HEADS * HEAD_DIM + CONV_CH) ** -0.5, 0.125, ((0, 4), (1, 8))),
        "out_conv": centred(splits[13], (CONV_CH, D), (Q_HEADS * HEAD_DIM + CONV_CH) ** -0.5, 0.125, ((0, 4), (1, 8))),
    }


EPS = 1e-06
ROPE_BASE = 10000.0
NEG_FILL = -1e+30

def normalize(values, gain):
    return values * lax.rsqrt(lax.optimization_barrier(jnp.mean(values * values, axis=-1, keepdims=True)) + EPS) * gain

def rotate(values, positions):
    half = values.shape[-1] // 2
    freq = ROPE_BASE ** (-jnp.arange(half, dtype=jnp.float32) / half)
    angle = positions[:, None] * freq
    cosine = jnp.cos(angle)[:, None, :]
    sine = jnp.sin(angle)[:, None, :]
    first = values[..., :half]
    second = values[..., half:]
    return jnp.concatenate([first * cosine - second * sine, second * cosine + first * sine], axis=-1)

def project(rows, weight):
    return lax.dot_general(rows, weight, (((1,), (1,)), ((), ())), preferred_element_type=jnp.float32).astype(jnp.bfloat16)

def reference(tokens, norm_gain, query_weight, key_weight, value_weight, gate_weight, left_weight, input_weight, query_gain, key_gain, sink_logit, conv_weight, out_attention, out_conv):
    count = tokens.shape[0]
    normed = normalize(tokens.astype(jnp.float32), norm_gain).astype(jnp.bfloat16)
    query = project(normed, query_weight).reshape(count, Q_HEADS, HEAD_DIM)
    keys = project(normed, key_weight).reshape(count, KV_HEADS, HEAD_DIM)
    values = project(normed, value_weight).reshape(count, KV_HEADS, HEAD_DIM)
    gate = project(normed, gate_weight)
    left = project(normed, left_weight)
    inputs = project(normed, input_weight)
    positions = jnp.arange(count, dtype=jnp.float32)
    query_rot = rotate(normalize(query.astype(jnp.float32), query_gain), positions).astype(jnp.bfloat16)
    key_rot = rotate(normalize(keys.astype(jnp.float32), key_gain), positions).astype(jnp.bfloat16)
    group = Q_HEADS // KV_HEADS
    span = BLOCK + 2 * WINDOW
    padded_keys = jnp.pad(key_rot, ((WINDOW, WINDOW), (0, 0), (0, 0)))
    padded_values = jnp.pad(values, ((WINDOW, WINDOW), (0, 0), (0, 0)))
    nblocks = count // BLOCK
    shaped = query_rot.reshape(nblocks, BLOCK, KV_HEADS, group, HEAD_DIM)
    sinks = sink_logit.reshape(KV_HEADS, group)[:, :, None]

    def one_block(packed):
        block_index, query_block = packed
        begin = block_index * BLOCK
        key_block = lax.dynamic_slice_in_dim(padded_keys, begin, span, 0)
        value_block = lax.dynamic_slice_in_dim(padded_values, begin, span, 0)
        scores = jnp.einsum('qkgd,nkd->kgqn', query_block.astype(jnp.float32), key_block.astype(jnp.float32)) * HEAD_DIM ** (-0.5)
        query_pos = begin + jnp.arange(BLOCK, dtype=jnp.int32)
        key_pos = begin - WINDOW + jnp.arange(span, dtype=jnp.int32)
        allowed = (jnp.abs(query_pos[:, None] - key_pos[None, :]) <= WINDOW) & (key_pos >= 0)[None, :] & (key_pos < count)[None, :]
        scores = jnp.where(allowed, scores, NEG_FILL)
        top = jnp.maximum(lax.optimization_barrier(jnp.max(scores, axis=-1)), sinks)
        expo = jnp.exp(scores - top[..., None])
        total = lax.optimization_barrier(jnp.sum(expo, axis=-1)) + jnp.exp(sinks - top)
        weights = (expo / total[..., None]).astype(jnp.bfloat16)
        return jnp.einsum('kgqn,nkd->qkgd', weights.astype(jnp.float32), value_block.astype(jnp.float32)).astype(jnp.bfloat16)
    attended = lax.map(one_block, (jnp.arange(nblocks, dtype=jnp.int32), shaped)).reshape(count, Q_HEADS * HEAD_DIM)
    product = (left.astype(jnp.float32) * inputs.astype(jnp.float32)).astype(jnp.bfloat16)
    padded = jnp.pad(product.astype(jnp.float32), ((1, 1), (0, 0)))
    convolved = conv_weight[0] * padded[:-2] + conv_weight[1] * padded[1:-1] + conv_weight[2] * padded[2:]
    gated = (gate.astype(jnp.float32) * convolved).astype(jnp.bfloat16)
    attn_width = Q_HEADS * HEAD_DIM // N_TP
    conv_width = CONV_CH // N_TP
    summed = jnp.zeros((count, D), jnp.float32)
    for place in range(N_TP):
        partial_sum = jnp.dot(attended[:, place * attn_width:(place + 1) * attn_width], out_attention[place * attn_width:(place + 1) * attn_width], preferred_element_type=jnp.float32)
        partial_sum = partial_sum + jnp.dot(gated[:, place * conv_width:(place + 1) * conv_width], out_conv[place * conv_width:(place + 1) * conv_width], preferred_element_type=jnp.float32)
        summed = summed + partial_sum.astype(jnp.bfloat16).astype(jnp.float32)
    return summed.astype(jnp.bfloat16)
```

```python
import functools

import jax
import jax.numpy as jnp
import numpy as np
from jax import lax
from jax.experimental import pallas as pl
from jax.experimental.pallas import tpu as pltpu
from jax.sharding import PartitionSpec as P

HEAD_DIM = 64
WINDOW = 128
BLOCK = 128


EPS = 1e-06
ROPE_BASE = 10000.0
NEG_FILL = -1e30


def with_halo(cells, sides, width):
    for axis, dim in sides:
        count = lax.axis_size(axis)
        ends = count - 1
        head = lax.slice_in_dim(cells, 0, width, axis=dim)
        tail = lax.slice_in_dim(cells, cells.shape[dim] - width, cells.shape[dim], axis=dim)
        cells = jnp.concatenate(
            [
                lax.ppermute(tail, axis, [(i, (i + 1) % count) for i in range(ends)]),
                cells,
                lax.ppermute(head, axis, [((i + 1) % count, i) for i in range(ends)]),
            ],
            axis=dim,
        )
    return cells


def normalize(values, gain):
    return values * lax.rsqrt(jnp.mean(values * values, axis=-1, keepdims=True) + EPS) * gain


def rotate(values, positions):
    half = values.shape[-1] // 2
    freq = ROPE_BASE ** (-jnp.arange(half, dtype=jnp.float32) / half)
    angle = positions[:, None] * freq
    cosine = jnp.cos(angle)[:, None, :]
    sine = jnp.sin(angle)[:, None, :]
    first = values[..., :half]
    second = values[..., half:]
    return jnp.concatenate(
        [first * cosine - second * sine, second * cosine + first * sine], axis=-1
    )


def project(rows, weight):
    return lax.dot_general(
        rows, weight, (((1,), (1,)), ((), ())), preferred_element_type=jnp.float32
    ).astype(jnp.bfloat16)


def attend(query_rot, key_rim, value_rim, sinks, offset, total):
    count = query_rot.shape[0]
    local_heads = query_rot.shape[1]
    kv_local = key_rim.shape[1]
    group = local_heads // kv_local
    span = BLOCK + 2 * WINDOW
    nblocks = count // BLOCK
    shaped = query_rot.reshape(nblocks, BLOCK, kv_local, group, HEAD_DIM)
    sink_group = sinks.reshape(kv_local, group)[:, :, None]

    def one_block(packed):
        block_index, query_block = packed
        begin = block_index * BLOCK
        key_block = lax.dynamic_slice_in_dim(key_rim, begin, span, 0)
        value_block = lax.dynamic_slice_in_dim(value_rim, begin, span, 0)
        scores = jnp.einsum(
            "qkgd,nkd->kgqn", query_block, key_block, preferred_element_type=jnp.float32
        ) * HEAD_DIM ** (-0.5)
        query_pos = offset + begin + jnp.arange(BLOCK, dtype=jnp.int32)
        key_pos = offset + begin - WINDOW + jnp.arange(span, dtype=jnp.int32)
        allowed = (
            (jnp.abs(query_pos[:, None] - key_pos[None, :]) <= WINDOW)
            & (key_pos >= 0)[None, :]
            & (key_pos < total)[None, :]
        )
        scores = jnp.where(allowed, scores, NEG_FILL)
        top = jnp.maximum(jnp.max(scores, axis=-1), sink_group)
        expo = jnp.exp(scores - top[..., None])
        denom = jnp.sum(expo, axis=-1) + jnp.exp(sink_group - top)
        weights = (expo / denom[..., None]).astype(jnp.bfloat16)
        return jnp.einsum(
            "kgqn,nkd->qkgd", weights, value_block, preferred_element_type=jnp.float32
        ).astype(jnp.bfloat16)

    result = lax.map(one_block, (jnp.arange(nblocks, dtype=jnp.int32), shaped))
    return result.reshape(count, local_heads * HEAD_DIM)


def per_device(
    tokens,
    norm_gain,
    query_weight,
    key_weight,
    value_weight,
    gate_weight,
    left_weight,
    input_weight,
    query_gain,
    key_gain,
    sink_logit,
    conv_weight,
    out_attention,
    out_conv,
):
    sp_count = lax.axis_size("sp")
    sp_place = lax.axis_index("sp")
    gathered = (
        lax.all_gather(query_weight, "sp", axis=1, tiled=True),
        lax.all_gather(key_weight, "sp", axis=1, tiled=True),
        lax.all_gather(value_weight, "sp", axis=1, tiled=True),
        lax.all_gather(gate_weight, "sp", axis=1, tiled=True),
        lax.all_gather(left_weight, "sp", axis=1, tiled=True),
        lax.all_gather(input_weight, "sp", axis=1, tiled=True),
        lax.all_gather(out_attention, "sp", axis=1, tiled=True),
        lax.all_gather(out_conv, "sp", axis=1, tiled=True),
    )
    (
        query_full,
        key_full,
        value_full,
        gate_full,
        left_full,
        input_full,
        attn_out_full,
        conv_out_full,
    ) = gathered
    normed = normalize(tokens.astype(jnp.float32), norm_gain).astype(jnp.bfloat16)
    widths = [
        query_full.shape[0],
        key_full.shape[0],
        value_full.shape[0],
        gate_full.shape[0],
        left_full.shape[0],
        input_full.shape[0],
    ]
    piece = lax.all_gather(normed, "tp", axis=0, tiled=True)
    joined = jnp.concatenate(
        [
            project(piece, weight)
            for weight in (query_full, key_full, value_full, gate_full, left_full, input_full)
        ],
        axis=1,
    )
    count = joined.shape[0]
    bounds = [0]
    for width in widths:
        bounds.append(bounds[-1] + width)
    query, keys, values, gate, left, inputs = [
        joined[:, bounds[place] : bounds[place + 1]] for place in range(6)
    ]
    offset = sp_place * count
    total = count * sp_count
    positions = (offset + jnp.arange(count, dtype=jnp.int32)).astype(jnp.float32)
    local_heads = widths[0] // HEAD_DIM
    kv_local = widths[1] // HEAD_DIM
    query_rot = rotate(
        normalize(query.reshape(count, local_heads, HEAD_DIM).astype(jnp.float32), query_gain),
        positions,
    ).astype(jnp.bfloat16)
    key_rot = rotate(
        normalize(keys.reshape(count, kv_local, HEAD_DIM).astype(jnp.float32), key_gain), positions
    ).astype(jnp.bfloat16)
    key_flat = key_rot.reshape(count, kv_local * HEAD_DIM)
    product = (left.astype(jnp.float32) * inputs.astype(jnp.float32)).astype(jnp.bfloat16)
    kv_width = widths[1]
    pair_rim = with_halo(jnp.concatenate([key_flat, values], axis=1), (("sp", 0),), WINDOW)
    product_rim = with_halo(product, (("sp", 0),), 1)
    rim_rows = pair_rim.shape[0]
    key_rim = pair_rim[:, :kv_width].reshape(rim_rows, kv_local, HEAD_DIM)
    value_rim = pair_rim[:, kv_width:].reshape(rim_rows, kv_local, HEAD_DIM)
    attended = attend(query_rot, key_rim, value_rim, sink_logit, offset, total)
    padded = product_rim.astype(jnp.float32)
    convolved = (
        conv_weight[0] * padded[:-2] + conv_weight[1] * padded[1:-1] + conv_weight[2] * padded[2:]
    )
    gated = (gate.astype(jnp.float32) * convolved).astype(jnp.bfloat16)
    return lax.psum_scatter(
        (
            jnp.dot(attended, attn_out_full, preferred_element_type=jnp.float32)
            + jnp.dot(gated, conv_out_full, preferred_element_type=jnp.float32)
        ).astype(jnp.bfloat16),
        "tp",
        scatter_dimension=0,
        tiled=True,
    )


MESH = pl.DeviceIdType.MESH


def fused_kernel(
    dims,
    tok_hbm, gain_ref, q_hbm, k_hbm, v_hbm, g_hbm, l_hbm, i_hbm,
    qgain_ref, kgain_ref, sink_ref, conv_ref, oa_hbm, oc_hbm, trig_hbm,
    out_ref,
    tok, trig, stage, ostage, win, wout, normed, acc, rim, mix, qrot,
    keep, s1, r1, s2, r2, s3, r3,
    local_sem, y_send, oy_send, in_recv, out_recv, in_up, in_down, out_up, out_down,
    tok_send, tok_recv, rim_send, rim_recv, rs_send, rs_recv,
):
    line, rows, depth, qr, kr, cr = (
        dims["line"], dims["rows"], dims["depth"], dims["qr"], dims["kr"], dims["cr"]
    )
    sp = lax.axis_index("sp")
    tp = lax.axis_index("tp")
    z, y = sp // 2, sp % 2
    x, c = tp // 2, tp % 2
    y_peer = (2 * z + 1 - y, tp)
    x_peer = (sp, 2 * (1 - x) + c)
    c_peer = (sp, 2 * x + 1 - c)
    up = (jnp.minimum(2 * (z + 1) + y, 2 * line - 1), tp)
    down = (jnp.maximum(2 * (z - 1) + y, 0), tp)
    has_up = z < line - 1
    has_down = z > 0
    s_own = sp
    s_mate = 2 * z + 1 - y
    plane = 8 * rows

    barrier = pltpu.get_barrier_semaphore()
    for peer in (y_peer, x_peer, c_peer):
        pl.semaphore_signal(barrier, inc=1, device_id=peer, device_id_type=MESH)

    @pl.when(has_up)
    def _():
        pl.semaphore_signal(barrier, inc=1, device_id=up, device_id_type=MESH)

    @pl.when(has_down)
    def _():
        pl.semaphore_signal(barrier, inc=1, device_id=down, device_id_type=MESH)

    counter = [0]

    def local(src, dst):
        copy = pltpu.make_async_copy(src, dst, local_sem.at[counter[0]])
        counter[0] += 1
        copy.start()
        return copy

    def pieces(which, dst):
        q0, c0 = pl.multiple_of(which * qr, qr), pl.multiple_of(which * cr, cr)
        return [
            local(q_hbm.at[pl.ds(q0, qr)], dst.at[0:qr]),
            local(k_hbm, dst.at[qr : qr + kr]),
            local(v_hbm, dst.at[qr + kr : qr + 2 * kr]),
            local(g_hbm.at[pl.ds(c0, cr)], dst.at[qr + 2 * kr : qr + 2 * kr + cr]),
            local(l_hbm.at[pl.ds(c0, cr)], dst.at[qr + 2 * kr + cr : qr + 2 * kr + 2 * cr]),
            local(i_hbm.at[pl.ds(c0, cr)], dst.at[qr + 2 * kr + 2 * cr : qr + 2 * kr + 3 * cr]),
        ]

    def out_pieces(which, dst):
        q0, c0 = pl.multiple_of(which * qr, qr), pl.multiple_of(which * cr, cr)
        return [
            local(oa_hbm.at[pl.ds(q0, qr)], dst.at[0:qr]),
            local(oc_hbm.at[pl.ds(c0, cr)], dst.at[qr : qr + cr]),
        ]

    mine = pieces(y, win.at[s_own])
    theirs = pieces(1 - y, stage)
    tok_copy = local(tok_hbm, tok)
    out_theirs = out_pieces(1 - y, ostage)
    out_mine = out_pieces(y, wout.at[s_own])
    trig_copy = local(trig_hbm.at[pl.ds(pl.multiple_of(z * plane, plane), plane)], trig)

    pl.semaphore_wait(barrier, 3 + has_up.astype(jnp.int32) + has_down.astype(jnp.int32))

    def remote(src, dst, send, recv, peer):
        return pltpu.make_async_remote_copy(
            src_ref=src, dst_ref=dst, send_sem=send, recv_sem=recv,
            device_id=peer, device_id_type=MESH,
        )

    def hop(buf, s, send, recv, peer):
        return remote(buf.at[s], buf.at[s], send.at[s], recv.at[s], peer)

    def forward(buf, s, source, ups, downs, recv):
        @pl.when((source <= z) & has_up)
        def _():
            hop(buf, s, ups, recv, up).start()

        @pl.when((source >= z) & has_down)
        def _():
            hop(buf, s, downs, recv, down).start()

    for copy in mine:
        copy.wait()
    forward(win, s_own, z, in_up, in_down, in_recv)
    for copy in theirs:
        copy.wait()
    y_copy = remote(stage, win.at[s_own], y_send.at[0], in_recv.at[s_own], y_peer)
    y_copy.start()
    tok_copy.wait()
    t = tok[...].astype(jnp.float32)
    t = t * lax.rsqrt(jnp.mean(t * t, axis=-1, keepdims=True) + EPS) * gain_ref[...]
    own_block = 4 * y + 2 * x + c
    normed[own_block] = t.astype(jnp.bfloat16)
    for copy in out_theirs:
        copy.wait()
    oy_copy = remote(ostage, wout.at[s_own], oy_send.at[0], out_recv.at[s_own], y_peer)
    oy_copy.start()
    for copy in out_mine:
        copy.wait()

    def block_of(yy, xx, cc):
        return 4 * yy + 2 * xx + cc

    def tok_hop(block, slot, peer):
        return remote(
            normed.at[block], normed.at[block], tok_send.at[slot], tok_recv.at[block], peer
        )

    xb = block_of(y, 1 - x, c)
    yb0 = block_of(1 - y, x, c)
    yb1 = block_of(1 - y, 1 - x, c)
    tok_copies = [
        tok_hop(own_block, 0, x_peer),
        tok_hop(own_block, 1, y_peer),
        tok_hop(own_block, 2, c_peer),
    ]
    for copy in tok_copies:
        copy.start()

    def tok_wait(block):
        tok_hop(block, 0, x_peer).wait_recv()

    tok_wait(xb)
    more = [tok_hop(xb, 3, y_peer), tok_hop(xb, 4, c_peer)]
    for copy in more:
        copy.start()
    tok_copies += more

    hop(win, s_mate, in_up, in_recv, up).wait_recv()
    forward(win, s_mate, z, in_up, in_down, in_recv)
    hop(wout, s_mate, out_up, out_recv, up).wait_recv()

    def own_out(flag_up, flag_down):
        for s in (s_own, s_mate):
            @pl.when(flag_up & has_up)
            def _():
                hop(wout, s, out_up, out_recv, up).start()

            @pl.when(flag_down & has_down)
            def _():
                hop(wout, s, out_down, out_recv, down).start()

    own_out(z == 0, z == line - 1)

    tok_wait(yb0)
    copy = tok_hop(yb0, 5, c_peer)
    copy.start()
    tok_copies.append(copy)
    tok_wait(yb1)
    copy = tok_hop(yb1, 6, c_peer)
    copy.start()
    tok_copies.append(copy)
    for yy in range(2):
        for xx in range(2):
            tok_wait(block_of(yy, xx, 1 - c))

    def columns(s):
        return pl.ds(pl.multiple_of(s * depth, depth), depth)

    def in_dot(s):
        a = normed[:, :, columns(s)].reshape(plane, depth)
        return lax.dot_general(
            a, win[s], (((1,), (1,)), ((), ())), preferred_element_type=jnp.float32
        )

    paired = jnp.minimum(z, line - 1 - z)
    below_longer = z > line - 1 - z

    def source_of(k):
        d = jnp.where(k <= 2 * paired, (k + 1) // 2, k - paired)
        below = jnp.where(k <= 2 * paired, k % 2 == 1, below_longer)
        return jnp.where(below, z - d, z + d)

    acc[...] = in_dot(s_own)
    acc[...] += in_dot(s_mate)

    def in_step(k, carry):
        source = source_of(k)
        for half in range(2):
            first = jnp.where(half == 0, y, 1 - y)
            s = 2 * source + first
            hop(win, s, in_up, in_recv, up).wait_recv()
            forward(win, s, source, in_up, in_down, in_recv)
            if half == 1:
                own_out(source == 0, source == line - 1)
            acc[...] += in_dot(s)
        return carry

    lax.fori_loop(1, line, in_step, 0)

    trig_copy.wait()
    lane = lax.broadcasted_iota(jnp.int32, (plane, qr), 1)
    half_dim = HEAD_DIM // 2
    table = trig[...]
    cos2 = jnp.where(lane < HEAD_DIM, table, pltpu.roll(table, HEAD_DIM, 1))
    sin2 = jnp.where(lane < HEAD_DIM, pltpu.roll(table, HEAD_DIM, 1), table)
    low = lane < HEAD_DIM
    first_half = lane % HEAD_DIM < half_dim

    def rot(v):
        partner = jnp.where(
            first_half, pltpu.roll(v, qr - half_dim, 1), pltpu.roll(v, half_dim, 1)
        )
        return v * cos2 + partner * sin2

    def bf(v):
        return v.astype(jnp.bfloat16).astype(jnp.float32)

    kv = bf(acc[:, qr : 2 * qr])
    ksq = jnp.sum(jnp.where(low, kv * kv, 0.0), axis=-1, keepdims=True) / HEAD_DIM
    kn = kv * lax.rsqrt(ksq + EPS) * kgain_ref[...]
    krot = rot(kn)
    rim[WINDOW : WINDOW + plane, 0:qr] = jnp.where(low, krot, kv).astype(jnp.bfloat16)
    base = 2 * qr
    left = bf(acc[:, base + cr : base + 2 * cr])
    inputs = bf(acc[:, base + 2 * cr : base + 3 * cr])
    rim[WINDOW : WINDOW + plane, qr : qr + cr] = (left * inputs).astype(jnp.bfloat16)

    qv = bf(acc[:, 0:qr])
    qq = qv * qv
    q_lo = jnp.sum(jnp.where(low, qq, 0.0), axis=-1, keepdims=True) / HEAD_DIM
    q_hi = jnp.sum(jnp.where(low, 0.0, qq), axis=-1, keepdims=True) / HEAD_DIM
    qn = qv * lax.rsqrt(jnp.where(low, q_lo, q_hi) + EPS) * qgain_ref[...]
    qro = rot(qn)

    bottom = pl.ds(WINDOW, WINDOW)
    top = pl.ds(plane, WINDOW)
    rim_up = remote(rim.at[top], rim.at[pl.ds(0, WINDOW)], rim_send.at[0], rim_recv.at[0], up)
    rim_down = remote(
        rim.at[bottom], rim.at[pl.ds(WINDOW + plane, WINDOW)], rim_send.at[1], rim_recv.at[1], down
    )

    @pl.when(has_up)
    def _():
        rim_up.start()

    @pl.when(has_down)
    def _():
        rim_down.start()

    zero_rim = jnp.zeros((WINDOW, qr + cr), jnp.bfloat16)

    @pl.when(z == 0)
    def _():
        rim[0:WINDOW] = zero_rim

    @pl.when(z == line - 1)
    def _():
        rim[WINDOW + plane :] = zero_rim

    qrot[0] = jnp.where(low, qro, 0.0).astype(jnp.bfloat16)
    qrot[1] = jnp.where(low, pltpu.roll(qro, HEAD_DIM, 1), 0.0).astype(jnp.bfloat16)

    @pl.when(has_down)
    def _():
        rim_up.wait_recv()

    @pl.when(has_up)
    def _():
        rim_down.wait_recv()

    span = BLOCK + 2 * WINDOW
    total = plane * line

    def att_step(block, carry):
        begin = pl.multiple_of(block * BLOCK, BLOCK)
        kvb = rim[pl.ds(begin, span), 0:qr]
        qb = qrot[:, pl.ds(begin, BLOCK), :].reshape(2 * BLOCK, qr)
        scores = lax.dot_general(
            qb, kvb, (((1,), (1,)), ((), ())), preferred_element_type=jnp.float32
        ) * HEAD_DIM ** (-0.5)
        row = lax.broadcasted_iota(jnp.int32, (2 * BLOCK, span), 0)
        col = lax.broadcasted_iota(jnp.int32, (2 * BLOCK, span), 1)
        gap = row % BLOCK + WINDOW - col
        pos = z * plane + begin - WINDOW + col
        allowed = (gap <= WINDOW) & (gap >= -WINDOW) & (pos >= 0) & (pos < total)
        scores = jnp.where(allowed, scores, NEG_FILL)
        head = lax.broadcasted_iota(jnp.int32, (2 * BLOCK, 1), 0)
        sink = jnp.where(head < BLOCK, sink_ref[0, 2 * y], sink_ref[0, 2 * y + 1])
        peak = jnp.maximum(jnp.max(scores, axis=-1, keepdims=True), sink)
        expo = jnp.exp(scores - peak)
        denom = jnp.sum(expo, axis=-1, keepdims=True) + jnp.exp(sink - peak)
        weights = (expo / denom).astype(jnp.bfloat16)
        o = jnp.dot(weights, kvb, preferred_element_type=jnp.float32)
        low_b = lax.broadcasted_iota(jnp.int32, (BLOCK, qr), 1) < HEAD_DIM
        both = jnp.where(low_b, pltpu.roll(o[:BLOCK], HEAD_DIM, 1), o[BLOCK:])
        mix[pl.ds(begin, BLOCK), 0:qr] = both.astype(jnp.bfloat16)
        return carry

    lax.fori_loop(0, plane // BLOCK, att_step, 0)

    extra = plane + 32
    p = rim[WINDOW - 16 : WINDOW + plane + 16, qr : qr + cr].astype(jnp.float32)
    taps = conv_ref[y]
    before = pltpu.roll(p, 1, 0)[16 : 16 + plane]
    after = pltpu.roll(p, extra - 1, 0)[16 : 16 + plane]
    convolved = taps[0:1] * before + taps[1:2] * p[16 : 16 + plane] + taps[2:3] * after
    gate = bf(acc[:, base : base + cr])
    mix[:, qr : qr + cr] = (gate * convolved).astype(jnp.bfloat16)

    def group(cc):
        return [
            mix[pl.ds(pl.multiple_of((2 * q + cc) * rows, rows), rows), :] for q in range(4)
        ]

    mine_rows = jnp.concatenate(group(c), axis=0)
    other_rows = jnp.concatenate(group(1 - c), axis=0)
    rs_copies = []

    def send_rs(src, dst, stage_id, s, peer):
        copy = remote(src, dst, rs_send.at[stage_id, s], rs_recv.at[stage_id, s], peer)
        copy.start()
        rs_copies.append(copy)

    def stage_a(k):
        source = z if k == 0 else source_of(jnp.int32(k))
        for half in range(2):
            s = 2 * source + half
            if k:
                hop(wout, s, out_up, out_recv, up).wait_recv()
                forward(wout, s, source, out_up, out_down, out_recv)
            weight = wout[s]
            s1[s] = jnp.dot(
                other_rows, weight, preferred_element_type=jnp.float32
            ).astype(jnp.bfloat16).reshape(2, 2, rows, depth)
            send_rs(s1.at[s], r1.at[s], 0, s, c_peer)
            keep[s] = jnp.dot(
                mine_rows, weight, preferred_element_type=jnp.float32
            ).reshape(2, 2, rows, depth)

    def axis_index_of(half):
        return (y, x) if half == 0 else (x, y)

    def stage_b(k):
        source = z if k == 0 else source_of(jnp.int32(k))
        for half in range(2):
            s = 2 * source + half
            remote(s1.at[s], r1.at[s], rs_send.at[0, s], rs_recv.at[0, s], c_peer).wait_recv()
            for j in range(2):
                if half == 0:
                    s2[s, j] = (keep[s, 1 - y, j] + r1[s, 1 - y, j].astype(jnp.float32)).astype(
                        jnp.bfloat16
                    )
                else:
                    s2[s, j] = (keep[s, j, 1 - x] + r1[s, j, 1 - x].astype(jnp.float32)).astype(
                        jnp.bfloat16
                    )
            send_rs(s2.at[s], r2.at[s], 1, s, y_peer if half == 0 else x_peer)

    def stage_c(k):
        source = z if k == 0 else source_of(jnp.int32(k))
        for half in range(2):
            s = 2 * source + half
            peer = y_peer if half == 0 else x_peer
            remote(s2.at[s], r2.at[s], rs_send.at[1, s], rs_recv.at[1, s], peer).wait_recv()
            my = x if half == 0 else y
            for own, j in ((False, 1 - my), (True, my)):
                if half == 0:
                    part = keep[s, y, j] + r1[s, y, j].astype(jnp.float32)
                else:
                    part = keep[s, j, x] + r1[s, j, x].astype(jnp.float32)
                part = part + r2[s, j].astype(jnp.float32)
                if own:
                    keep[s, y, x] = part
                else:
                    s3[s] = part.astype(jnp.bfloat16)
                    send_rs(s3.at[s], r3.at[s], 2, s, x_peer if half == 0 else y_peer)

    def stage_d(k):
        source = z if k == 0 else source_of(jnp.int32(k))
        for half in range(2):
            s = 2 * source + half
            peer = x_peer if half == 0 else y_peer
            remote(s3.at[s], r3.at[s], rs_send.at[2, s], rs_recv.at[2, s], peer).wait_recv()
            out_ref[:, columns(s)] = (keep[s, y, x] + r3[s].astype(jnp.float32)).astype(
                jnp.bfloat16
            )

    for k in range(line):
        stage_a(k)
        if k >= 1:
            stage_c(k - 1)
        stage_b(k)
        if k >= 1:
            stage_d(k - 1)
    stage_c(line - 1)
    stage_d(line - 1)

    for copy in [y_copy, oy_copy] + tok_copies + rs_copies:
        copy.wait_send()

    @pl.when(has_up)
    def _():
        rim_up.wait_send()

    @pl.when(has_down)
    def _():
        rim_down.wait_send()

    for s in range(2 * line):
        for buf, ups, downs, recv in (
            (win, in_up, in_down, in_recv), (wout, out_up, out_down, out_recv)
        ):
            @pl.when((s // 2 <= z) & has_up)
            def _():
                hop(buf, s, ups, recv, up).wait_send()

            @pl.when((s // 2 >= z) & has_down)
            def _():
                hop(buf, s, downs, recv, down).wait_send()


def trig_table(total):
    half = HEAD_DIM // 2
    freq = np.float64(ROPE_BASE) ** (-np.arange(half) / half)
    angle = np.arange(total)[:, None] * freq
    cosine, sine = np.cos(angle), np.sin(angle)
    return np.concatenate([cosine, cosine, -sine, sine], axis=1).astype(np.float32)


def fused_device(
    tokens, norm_gain, query_weight, key_weight, value_weight, gate_weight, left_weight,
    input_weight, query_gain, key_gain, sink_logit, conv_weight, out_attention, out_conv,
):
    sp_count = lax.axis_size("sp")
    line = sp_count // 2
    rows, width = tokens.shape
    depth = query_weight.shape[1]
    qr = query_weight.shape[0] // 2
    kr = key_weight.shape[0]
    cr = gate_weight.shape[0] // 2
    fan = qr + 2 * kr + 3 * cr
    plane = 8 * rows
    dims = dict(line=line, rows=rows, depth=depth, qr=qr, kr=kr, cr=cr)
    vm = pl.BlockSpec(memory_space=pltpu.VMEM)
    sm = pl.BlockSpec(memory_space=pltpu.SMEM)
    hb = pl.BlockSpec(memory_space=pl.ANY)
    bf16, f32 = jnp.bfloat16, jnp.float32
    dma = pltpu.SemaphoreType.DMA
    n = sp_count
    scratch = [
        pltpu.VMEM((rows, width), bf16),
        pltpu.VMEM((plane, 2 * HEAD_DIM), f32),
        pltpu.VMEM((fan, depth), bf16),
        pltpu.VMEM((qr + cr, depth), bf16),
        pltpu.VMEM((n, fan, depth), bf16),
        pltpu.VMEM((n, qr + cr, depth), bf16),
        pltpu.VMEM((8, rows, width), bf16),
        pltpu.VMEM((plane, fan), f32),
        pltpu.VMEM((plane + 2 * WINDOW, qr + cr), bf16),
        pltpu.VMEM((plane, qr + cr), bf16),
        pltpu.VMEM((2, plane, qr), bf16),
        pltpu.VMEM((n, 2, 2, rows, depth), f32),
        pltpu.VMEM((n, 2, 2, rows, depth), bf16),
        pltpu.VMEM((n, 2, 2, rows, depth), bf16),
        pltpu.VMEM((n, 2, rows, depth), bf16),
        pltpu.VMEM((n, 2, rows, depth), bf16),
        pltpu.VMEM((n, rows, depth), bf16),
        pltpu.VMEM((n, rows, depth), bf16),
        dma((18,)), dma((1,)), dma((1,)), dma((n,)), dma((n,)),
        dma((n,)), dma((n,)), dma((n,)), dma((n,)),
        dma((7,)), dma((8,)), dma((2,)), dma((2,)), dma((3, n)), dma((3, n)),
    ]
    taps = conv_weight.reshape(3, 2, cr).transpose(1, 0, 2)
    return pl.pallas_call(
        functools.partial(fused_kernel, dims),
        out_shape=jax.ShapeDtypeStruct((rows, width), bf16),
        in_specs=[hb, vm, hb, hb, hb, hb, hb, hb, vm, vm, sm, vm, hb, hb, hb],
        out_specs=vm,
        scratch_shapes=scratch,
        compiler_params=pltpu.CompilerParams(
            collective_id=0, has_side_effects=True, vmem_limit_bytes=56 * 1024 * 1024
        ),
    )(
        tokens, norm_gain[None, :], query_weight, key_weight, value_weight, gate_weight,
        left_weight, input_weight, jnp.tile(query_gain, 2)[None, :],
        jnp.tile(key_gain, 2)[None, :], sink_logit[None, :], taps, out_attention, out_conv,
        jnp.asarray(trig_table(plane * line)),
    )


def local_device(*args):
    tokens, query_weight, key_weight, gate_weight = args[0], args[2], args[3], args[5]
    fits = (
        lax.axis_size("sp") % 2 == 0
        and lax.axis_size("sp") <= 16
        and lax.axis_size("tp") == 4
        and query_weight.shape[1] % 128 == 0
        and query_weight.shape[0] == 4 * HEAD_DIM
        and key_weight.shape[0] == HEAD_DIM
        and gate_weight.shape[0] == 256
        and tokens.shape[0] % 16 == 0
        and 8 * tokens.shape[0] % BLOCK == 0
    )
    return fused_device(*args) if fits else per_device(*args)


def solution(mesh):
    in_specs = (
        P(("sp", "tp"), None),
        P(),
        P("tp", "sp"),
        P("tp", "sp"),
        P("tp", "sp"),
        P("tp", "sp"),
        P("tp", "sp"),
        P("tp", "sp"),
        P(),
        P(),
        P("tp"),
        P(None, "tp"),
        P("tp", "sp"),
        P("tp", "sp"),
    )
    out_specs = P(("sp", "tp"), None)
    return jax.shard_map(
        local_device, mesh=mesh, in_specs=in_specs, out_specs=out_specs, check_vma=False
    )
```

```python
import functools

import jax
import jax.numpy as jnp
import numpy as np
from jax import lax
from jax.experimental import pallas as pl
from jax.experimental.pallas import tpu as pltpu
from jax.sharding import PartitionSpec as P

HEAD_DIM = 64
WINDOW = 128
BLOCK = 128


EPS = 1e-06
ROPE_BASE = 10000.0
NEG_FILL = -1e30


def with_halo(cells, sides, width):
    for axis, dim in sides:
        count = lax.axis_size(axis)
        ends = count - 1
        head = lax.slice_in_dim(cells, 0, width, axis=dim)
        tail = lax.slice_in_dim(cells, cells.shape[dim] - width, cells.shape[dim], axis=dim)
        cells = jnp.concatenate(
            [
                lax.ppermute(tail, axis, [(i, (i + 1) % count) for i in range(ends)]),
                cells,
                lax.ppermute(head, axis, [((i + 1) % count, i) for i in range(ends)]),
            ],
            axis=dim,
        )
    return cells


def normalize(values, gain):
    return values * lax.rsqrt(jnp.mean(values * values, axis=-1, keepdims=True) + EPS) * gain


def rotate(values, positions):
    half = values.shape[-1] // 2
    freq = ROPE_BASE ** (-jnp.arange(half, dtype=jnp.float32) / half)
    angle = positions[:, None] * freq
    cosine = jnp.cos(angle)[:, None, :]
    sine = jnp.sin(angle)[:, None, :]
    first = values[..., :half]
    second = values[..., half:]
    return jnp.concatenate(
        [first * cosine - second * sine, second * cosine + first * sine], axis=-1
    )


def project(rows, weight):
    return lax.dot_general(
        rows, weight, (((1,), (1,)), ((), ())), preferred_element_type=jnp.float32
    ).astype(jnp.bfloat16)


def attend(query_rot, key_rim, value_rim, sinks, offset, total):
    count = query_rot.shape[0]
    local_heads = query_rot.shape[1]
    kv_local = key_rim.shape[1]
    group = local_heads // kv_local
    span = BLOCK + 2 * WINDOW
    nblocks = count // BLOCK
    shaped = query_rot.reshape(nblocks, BLOCK, kv_local, group, HEAD_DIM)
    sink_group = sinks.reshape(kv_local, group)[:, :, None]

    def one_block(packed):
        block_index, query_block = packed
        begin = block_index * BLOCK
        key_block = lax.dynamic_slice_in_dim(key_rim, begin, span, 0)
        value_block = lax.dynamic_slice_in_dim(value_rim, begin, span, 0)
        scores = jnp.einsum(
            "qkgd,nkd->kgqn", query_block, key_block, preferred_element_type=jnp.float32
        ) * HEAD_DIM ** (-0.5)
        query_pos = offset + begin + jnp.arange(BLOCK, dtype=jnp.int32)
        key_pos = offset + begin - WINDOW + jnp.arange(span, dtype=jnp.int32)
        allowed = (
            (jnp.abs(query_pos[:, None] - key_pos[None, :]) <= WINDOW)
            & (key_pos >= 0)[None, :]
            & (key_pos < total)[None, :]
        )
        scores = jnp.where(allowed, scores, NEG_FILL)
        top = jnp.maximum(jnp.max(scores, axis=-1), sink_group)
        expo = jnp.exp(scores - top[..., None])
        denom = jnp.sum(expo, axis=-1) + jnp.exp(sink_group - top)
        weights = (expo / denom[..., None]).astype(jnp.bfloat16)
        return jnp.einsum(
            "kgqn,nkd->qkgd", weights, value_block, preferred_element_type=jnp.float32
        ).astype(jnp.bfloat16)

    result = lax.map(one_block, (jnp.arange(nblocks, dtype=jnp.int32), shaped))
    return result.reshape(count, local_heads * HEAD_DIM)


def per_device(
    tokens,
    norm_gain,
    query_weight,
    key_weight,
    value_weight,
    gate_weight,
    left_weight,
    input_weight,
    query_gain,
    key_gain,
    sink_logit,
    conv_weight,
    out_attention,
    out_conv,
):
    sp_count = lax.axis_size("sp")
    sp_place = lax.axis_index("sp")
    gathered = (
        lax.all_gather(query_weight, "sp", axis=1, tiled=True),
        lax.all_gather(key_weight, "sp", axis=1, tiled=True),
        lax.all_gather(value_weight, "sp", axis=1, tiled=True),
        lax.all_gather(gate_weight, "sp", axis=1, tiled=True),
        lax.all_gather(left_weight, "sp", axis=1, tiled=True),
        lax.all_gather(input_weight, "sp", axis=1, tiled=True),
        lax.all_gather(out_attention, "sp", axis=1, tiled=True),
        lax.all_gather(out_conv, "sp", axis=1, tiled=True),
    )
    (
        query_full,
        key_full,
        value_full,
        gate_full,
        left_full,
        input_full,
        attn_out_full,
        conv_out_full,
    ) = gathered
    normed = normalize(tokens.astype(jnp.float32), norm_gain).astype(jnp.bfloat16)
    widths = [
        query_full.shape[0],
        key_full.shape[0],
        value_full.shape[0],
        gate_full.shape[0],
        left_full.shape[0],
        input_full.shape[0],
    ]
    piece = lax.all_gather(normed, "tp", axis=0, tiled=True)
    joined = jnp.concatenate(
        [
            project(piece, weight)
            for weight in (query_full, key_full, value_full, gate_full, left_full, input_full)
        ],
        axis=1,
    )
    count = joined.shape[0]
    bounds = [0]
    for width in widths:
        bounds.append(bounds[-1] + width)
    query, keys, values, gate, left, inputs = [
        joined[:, bounds[place] : bounds[place + 1]] for place in range(6)
    ]
    offset = sp_place * count
    total = count * sp_count
    positions = (offset + jnp.arange(count, dtype=jnp.int32)).astype(jnp.float32)
    local_heads = widths[0] // HEAD_DIM
    kv_local = widths[1] // HEAD_DIM
    query_rot = rotate(
        normalize(query.reshape(count, local_heads, HEAD_DIM).astype(jnp.float32), query_gain),
        positions,
    ).astype(jnp.bfloat16)
    key_rot = rotate(
        normalize(keys.reshape(count, kv_local, HEAD_DIM).astype(jnp.float32), key_gain), positions
    ).astype(jnp.bfloat16)
    key_flat = key_rot.reshape(count, kv_local * HEAD_DIM)
    product = (left.astype(jnp.float32) * inputs.astype(jnp.float32)).astype(jnp.bfloat16)
    kv_width = widths[1]
    pair_rim = with_halo(jnp.concatenate([key_flat, values], axis=1), (("sp", 0),), WINDOW)
    product_rim = with_halo(product, (("sp", 0),), 1)
    rim_rows = pair_rim.shape[0]
    key_rim = pair_rim[:, :kv_width].reshape(rim_rows, kv_local, HEAD_DIM)
    value_rim = pair_rim[:, kv_width:].reshape(rim_rows, kv_local, HEAD_DIM)
    attended = attend(query_rot, key_rim, value_rim, sink_logit, offset, total)
    padded = product_rim.astype(jnp.float32)
    convolved = (
        conv_weight[0] * padded[:-2] + conv_weight[1] * padded[1:-1] + conv_weight[2] * padded[2:]
    )
    gated = (gate.astype(jnp.float32) * convolved).astype(jnp.bfloat16)
    return lax.psum_scatter(
        (
            jnp.dot(attended, attn_out_full, preferred_element_type=jnp.float32)
            + jnp.dot(gated, conv_out_full, preferred_element_type=jnp.float32)
        ).astype(jnp.bfloat16),
        "tp",
        scatter_dimension=0,
        tiled=True,
    )


MESH = pl.DeviceIdType.MESH


def fused_kernel(
    dims,
    tok_hbm, gain_ref, q_hbm, k_hbm, v_hbm, g_hbm, l_hbm, i_hbm,
    qgain_ref, kgain_ref, sink_ref, conv_ref, oa_hbm, oc_hbm, trig_hbm,
    out_ref,
    tok, trig, stage, ostage, win, wout, normed, normed2, acc, acc2, rim, prod, prod2, mix_a, mix_c, gated2,
    qrot,
    keep, s1, r1, s2, r2, s3, r3,
    local_sem, y_send, oy_send, in_recv, out_recv, in_up, in_down, out_up, out_down,
    tok_send, tok_recv, tok2_send, tok2_recv, rim_send, rim_recv, prod_send, prod_recv, g_send, g_recv,
    rs_send, rs_recv,
):
    line, rows, depth, qr, kr, cr = (
        dims["line"], dims["rows"], dims["depth"], dims["qr"], dims["kr"], dims["cr"]
    )
    sp = lax.axis_index("sp")
    tp = lax.axis_index("tp")
    z, y = sp // 2, sp % 2
    x, c = tp // 2, tp % 2
    y_peer = (2 * z + 1 - y, tp)
    x_peer = (sp, 2 * (1 - x) + c)
    c_peer = (sp, 2 * x + 1 - c)
    up = (jnp.minimum(2 * (z + 1) + y, 2 * line - 1), tp)
    down = (jnp.maximum(2 * (z - 1) + y, 0), tp)
    has_up = z < line - 1
    has_down = z > 0
    s_own = sp
    s_mate = 2 * z + 1 - y
    plane = 8 * rows
    core = qr + 2 * kr
    is_end = (z == 0) | (z == line - 1)
    not_end = (z > 0) & (z < line - 1)
    is_help = (z == 1) | (z == line - 2)
    help_dev = (jnp.where(z == 0, 2 + y, 2 * (line - 2) + y), tp)
    end_dev = (jnp.where(z == 1, y, 2 * (line - 1) + y), tp)

    barrier = pltpu.get_barrier_semaphore()
    for peer in (y_peer, x_peer, c_peer):
        pl.semaphore_signal(barrier, inc=1, device_id=peer, device_id_type=MESH)

    @pl.when(has_up)
    def _():
        pl.semaphore_signal(barrier, inc=1, device_id=up, device_id_type=MESH)

    @pl.when(has_down)
    def _():
        pl.semaphore_signal(barrier, inc=1, device_id=down, device_id_type=MESH)

    counter = [0]

    def local(src, dst):
        copy = pltpu.make_async_copy(src, dst, local_sem.at[counter[0]])
        counter[0] += 1
        copy.start()
        return copy

    def pieces(which, dst):
        q0, c0 = pl.multiple_of(which * qr, qr), pl.multiple_of(which * cr, cr)
        return [
            local(q_hbm.at[pl.ds(q0, qr)], dst.at[0:qr]),
            local(k_hbm, dst.at[qr : qr + kr]),
            local(v_hbm, dst.at[qr + kr : qr + 2 * kr]),
            local(g_hbm.at[pl.ds(c0, cr)], dst.at[qr + 2 * kr : qr + 2 * kr + cr]),
            local(l_hbm.at[pl.ds(c0, cr)], dst.at[qr + 2 * kr + cr : qr + 2 * kr + 2 * cr]),
            local(i_hbm.at[pl.ds(c0, cr)], dst.at[qr + 2 * kr + 2 * cr : qr + 2 * kr + 3 * cr]),
        ]

    def out_pieces(which, dst):
        q0, c0 = pl.multiple_of(which * qr, qr), pl.multiple_of(which * cr, cr)
        return [
            local(oa_hbm.at[pl.ds(q0, qr)], dst.at[0:qr]),
            local(oc_hbm.at[pl.ds(c0, cr)], dst.at[qr : qr + cr]),
        ]

    mine = pieces(y, win.at[s_own])
    theirs = pieces(1 - y, stage)
    tok_copy = local(tok_hbm, tok)
    out_theirs = out_pieces(1 - y, ostage)
    out_mine = out_pieces(y, wout.at[s_own])
    trig_copy = local(trig_hbm.at[pl.ds(pl.multiple_of(z * plane, plane), plane)], trig)

    pl.semaphore_wait(barrier, 3 + has_up.astype(jnp.int32) + has_down.astype(jnp.int32))

    def remote(src, dst, send, recv, peer):
        return pltpu.make_async_remote_copy(
            src_ref=src, dst_ref=dst, send_sem=send, recv_sem=recv,
            device_id=peer, device_id_type=MESH,
        )

    def hop(buf, s, send, recv, peer):
        return remote(buf.at[s], buf.at[s], send.at[s], recv.at[s], peer)

    def trim_hop(s, send, peer):
        return remote(
            win.at[s, 0:core], win.at[s, 0:core], send.at[s], in_recv.at[s], peer
        )

    up_full = z + 1 < line - 1
    up_trim = z + 1 == line - 1
    down_full = z - 1 > 0
    down_trim = z - 1 == 0

    def in_sends(s, source, act):
        for full, trim, way, send, peer in (
            (up_full, up_trim, source <= z, in_up, up),
            (down_full, down_trim, source >= z, in_down, down),
        ):
            @pl.when(way & full)
            def _():
                act(hop(win, s, send, in_recv, peer))

            @pl.when(way & trim)
            def _():
                act(trim_hop(s, send, peer))

    def in_forward(s, source):
        in_sends(s, source, lambda copy: copy.start())

    def in_wait(s):
        @pl.when(is_end)
        def _():
            trim_hop(s, in_up, up).wait_recv()

        @pl.when(not_end)
        def _():
            hop(win, s, in_up, in_recv, up).wait_recv()

    def forward(buf, s, source, ups, downs, recv):
        @pl.when((source <= z) & has_up)
        def _():
            hop(buf, s, ups, recv, up).start()

        @pl.when((source >= z) & has_down)
        def _():
            hop(buf, s, downs, recv, down).start()

    for copy in mine:
        copy.wait()
    in_forward(s_own, z)
    for copy in theirs:
        copy.wait()
    y_copy = remote(stage, win.at[s_own], y_send.at[0], in_recv.at[s_own], y_peer)
    y_copy.start()
    tok_copy.wait()
    t = tok[...].astype(jnp.float32)
    t = t * lax.rsqrt(jnp.mean(t * t, axis=-1, keepdims=True) + EPS) * gain_ref[...]
    own_block = 4 * y + 2 * x + c
    normed[own_block] = t.astype(jnp.bfloat16)

    def end_tok(block, slot):
        return remote(
            normed.at[block], normed2.at[block], tok2_send.at[slot], tok2_recv.at[block], help_dev
        )

    def tok2_hop(block, slot, peer):
        return remote(
            normed2.at[block], normed2.at[block], tok2_send.at[slot], tok2_recv.at[block], peer
        )

    for copy in out_theirs:
        copy.wait()
    oy_copy = remote(ostage, wout.at[s_own], oy_send.at[0], out_recv.at[s_own], y_peer)
    oy_copy.start()
    for copy in out_mine:
        copy.wait()

    @pl.when(is_end)
    def _():
        end_tok(own_block, 0).start()

    def block_of(yy, xx, cc):
        return 4 * yy + 2 * xx + cc

    def tok_hop(block, slot, peer):
        return remote(
            normed.at[block], normed.at[block], tok_send.at[slot], tok_recv.at[block], peer
        )

    xb = block_of(y, 1 - x, c)
    yb0 = block_of(1 - y, x, c)
    yb1 = block_of(1 - y, 1 - x, c)
    tok_copies = [
        tok_hop(own_block, 0, x_peer),
        tok_hop(own_block, 1, y_peer),
        tok_hop(own_block, 2, c_peer),
    ]
    for copy in tok_copies:
        copy.start()

    def tok_wait(block):
        tok_hop(block, 0, x_peer).wait_recv()

    tok_wait(xb)
    more = [tok_hop(xb, 3, y_peer), tok_hop(xb, 4, c_peer)]
    for copy in more:
        copy.start()
    tok_copies += more

    hop(win, s_mate, in_up, in_recv, up).wait_recv()
    in_forward(s_mate, z)
    hop(wout, s_mate, out_up, out_recv, up).wait_recv()

    def own_out(flag_up, flag_down):
        for s in (s_own, s_mate):
            @pl.when(flag_up & has_up)
            def _():
                hop(wout, s, out_up, out_recv, up).start()

            @pl.when(flag_down & has_down)
            def _():
                hop(wout, s, out_down, out_recv, down).start()

    tok_wait(yb0)

    @pl.when(is_end)
    def _():
        end_tok(yb0, 1).start()

    own_out(z == 0, z == line - 1)
    copy = tok_hop(yb0, 5, c_peer)
    copy.start()
    tok_copies.append(copy)
    tok_wait(yb1)
    copy = tok_hop(yb1, 6, c_peer)
    copy.start()
    tok_copies.append(copy)
    for yy in range(2):
        for xx in range(2):
            tok_wait(block_of(yy, xx, 1 - c))

    def columns(s):
        return pl.ds(pl.multiple_of(s * depth, depth), depth)

    def dot_t(a, w):
        return lax.dot_general(a, w, (((1,), (1,)), ((), ())), preferred_element_type=jnp.float32)

    def in_dot(s, first):
        a = normed[:, :, columns(s)].reshape(plane, depth)
        low_part = dot_t(a, win[s, 0:core])
        acc[:, 0:core] = low_part if first else acc[:, 0:core] + low_part

        @pl.when(not_end)
        def _():
            high_part = dot_t(a, win[s, core:])
            acc[:, core:] = high_part if first else acc[:, core:] + high_part

    paired = jnp.minimum(z, line - 1 - z)
    below_longer = z > line - 1 - z

    def source_of(k):
        d = jnp.where(k <= 2 * paired, (k + 1) // 2, k - paired)
        below = jnp.where(k <= 2 * paired, k % 2 == 1, below_longer)
        return jnp.where(below, z - d, z + d)

    in_dot(s_own, True)
    in_dot(s_mate, False)

    def in_step(k, carry):
        source = source_of(k)
        for turn, block, slot in ((2, own_block, 2), (line - 1, yb0, 4)):
            @pl.when(is_help & (k == turn))
            def _():
                tok2_hop(block, slot, end_dev).wait_recv()
                tok2_hop(block, slot, x_peer).start()
                tok2_hop(block, slot + 1, c_peer).start()

        for half in range(2):
            first = jnp.where(half == 0, y, 1 - y)
            s = 2 * source + first
            in_wait(s)
            in_forward(s, source)
            if half == 1:
                own_out(source == 0, source == line - 1)
            in_dot(s, False)
        return carry

    lax.fori_loop(1, line, in_step, 0)

    trig_copy.wait()
    lane = lax.broadcasted_iota(jnp.int32, (plane, qr), 1)
    half_dim = HEAD_DIM // 2
    table = trig[...]
    cos2 = jnp.where(lane < HEAD_DIM, table, pltpu.roll(table, HEAD_DIM, 1))
    sin2 = jnp.where(lane < HEAD_DIM, pltpu.roll(table, HEAD_DIM, 1), table)
    low = lane < HEAD_DIM
    first_half = lane % HEAD_DIM < half_dim

    def rot(v):
        partner = jnp.where(
            first_half, pltpu.roll(v, qr - half_dim, 1), pltpu.roll(v, half_dim, 1)
        )
        return v * cos2 + partner * sin2

    def bf(v):
        return v.astype(jnp.bfloat16).astype(jnp.float32)

    kv = bf(acc[:, qr : 2 * qr])
    ksq = jnp.sum(jnp.where(low, kv * kv, 0.0), axis=-1, keepdims=True) / HEAD_DIM
    kgain = jnp.concatenate([kgain_ref[...], kgain_ref[...]], axis=1)
    kn = kv * lax.rsqrt(ksq + EPS) * kgain
    krot = rot(kn)
    rim[WINDOW : WINDOW + plane, :] = jnp.where(low, krot, kv).astype(jnp.bfloat16)
    base = 2 * qr

    qv = bf(acc[:, 0:qr])
    qq = qv * qv
    q_lo = jnp.sum(jnp.where(low, qq, 0.0), axis=-1, keepdims=True) / HEAD_DIM
    q_hi = jnp.sum(jnp.where(low, 0.0, qq), axis=-1, keepdims=True) / HEAD_DIM
    qgain = jnp.concatenate([qgain_ref[...], qgain_ref[...]], axis=1)
    qn = qv * lax.rsqrt(jnp.where(low, q_lo, q_hi) + EPS) * qgain
    qro = rot(qn)

    bottom = pl.ds(WINDOW, WINDOW)
    top = pl.ds(plane, WINDOW)
    rim_up = remote(rim.at[top], rim.at[pl.ds(0, WINDOW)], rim_send.at[0], rim_recv.at[0], up)
    rim_down = remote(
        rim.at[bottom], rim.at[pl.ds(WINDOW + plane, WINDOW)], rim_send.at[1], rim_recv.at[1], down
    )

    @pl.when(has_up)
    def _():
        rim_up.start()

    @pl.when(has_down)
    def _():
        rim_down.start()

    zero_rim = jnp.zeros((WINDOW, qr), jnp.bfloat16)

    @pl.when(z == 0)
    def _():
        rim[0:WINDOW] = zero_rim

    @pl.when(z == line - 1)
    def _():
        rim[WINDOW + plane :] = zero_rim

    qrot[0] = jnp.where(low, qro, 0.0).astype(jnp.bfloat16)
    qrot[1] = jnp.where(low, pltpu.roll(qro, HEAD_DIM, 1), 0.0).astype(jnp.bfloat16)

    pad = 16
    zero_pad = jnp.zeros((pad, cr), jnp.bfloat16)
    taps = conv_ref[y]

    def convolve(ref, gate):
        p = ref[...].astype(jnp.float32)
        before = pltpu.roll(p, 1, 0)[pad : pad + plane]
        after = pltpu.roll(p, plane + 2 * pad - 1, 0)[pad : pad + plane]
        mixed = taps[0:1] * before + taps[1:2] * p[pad : pad + plane] + taps[2:3] * after
        return (gate * mixed).astype(jnp.bfloat16)

    prod_up = remote(
        prod.at[pl.ds(plane, pad)], prod.at[pl.ds(0, pad)], prod_send.at[0], prod_recv.at[0], up
    )
    prod_down = remote(
        prod.at[pl.ds(pad, pad)], prod.at[pl.ds(pad + plane, pad)],
        prod_send.at[1], prod_recv.at[1], down,
    )
    from_up = not_end & up_full
    from_down = not_end & down_full

    @pl.when(not_end)
    def _():
        left = bf(acc[:, base + cr : base + 2 * cr])
        inputs = bf(acc[:, base + 2 * cr : base + 3 * cr])
        prod[pad : pad + plane] = (left * inputs).astype(jnp.bfloat16)

    @pl.when(from_up)
    def _():
        prod_up.start()

    @pl.when(from_down)
    def _():
        prod_down.start()

    g_copy = remote(gated2, mix_c, g_send.at[0], g_recv.at[0], end_dev)

    @pl.when(is_help)
    def _():
        for block, slot in ((xb, 6), (yb1, 7)):
            tok2_hop(block, slot, x_peer).wait_recv()
            tok2_hop(block, slot, c_peer).start()
        for yy in range(2):
            for xx in range(2):
                tok2_hop(block_of(yy, xx, 1 - c), 0, c_peer).wait_recv()
        acc2[...] = jnp.zeros_like(acc2)

        def help_step(s, carry):
            a = normed2[:, :, columns(s)].reshape(plane, depth)
            acc2[...] += dot_t(a, win[s, core:])
            return carry

        lax.fori_loop(0, 2 * line, help_step, 0)
        prod2[pad : pad + plane] = (
            bf(acc2[:, cr : 2 * cr]) * bf(acc2[:, 2 * cr : 3 * cr])
        ).astype(jnp.bfloat16)

        @pl.when(z == 1)
        def _():
            prod2[0:pad] = zero_pad
            prod2[pad + plane :] = prod[pad : 2 * pad]
            prod[0:pad] = prod2[plane : plane + pad]

        @pl.when(z != 1)
        def _():
            prod2[0:pad] = prod[plane : plane + pad]
            prod2[pad + plane :] = zero_pad
            prod[pad + plane :] = prod2[pad : 2 * pad]

        gated2[...] = convolve(prod2, bf(acc2[:, 0:cr]))
        g_copy.start()

    @pl.when(from_up)
    def _():
        prod_down.wait_recv()

    @pl.when(from_down)
    def _():
        prod_up.wait_recv()

    @pl.when(not_end)
    def _():
        mix_c[...] = convolve(prod, bf(acc[:, base : base + cr]))

    @pl.when(has_down)
    def _():
        rim_up.wait_recv()

    @pl.when(has_up)
    def _():
        rim_down.wait_recv()

    span = BLOCK + 2 * WINDOW
    total = plane * line

    def att_step(block, carry):
        begin = pl.multiple_of(block * BLOCK, BLOCK)
        kvb = rim[pl.ds(begin, span), :]
        qb = qrot[:, pl.ds(begin, BLOCK), :].reshape(2 * BLOCK, qr)
        scores = lax.dot_general(
            qb, kvb, (((1,), (1,)), ((), ())), preferred_element_type=jnp.float32
        ) * HEAD_DIM ** (-0.5)
        row = lax.broadcasted_iota(jnp.int32, (2 * BLOCK, span), 0)
        col = lax.broadcasted_iota(jnp.int32, (2 * BLOCK, span), 1)
        gap = row % BLOCK + WINDOW - col
        pos = z * plane + begin - WINDOW + col
        allowed = (gap <= WINDOW) & (gap >= -WINDOW) & (pos >= 0) & (pos < total)
        scores = jnp.where(allowed, scores, NEG_FILL)
        head = lax.broadcasted_iota(jnp.int32, (2 * BLOCK, 1), 0)
        sink = jnp.where(head < BLOCK, sink_ref[0, 2 * y], sink_ref[0, 2 * y + 1])
        peak = jnp.maximum(jnp.max(scores, axis=-1, keepdims=True), sink)
        expo = jnp.exp(scores - peak)
        denom = jnp.sum(expo, axis=-1, keepdims=True) + jnp.exp(sink - peak)
        weights = (expo / denom).astype(jnp.bfloat16)
        o = jnp.dot(weights, kvb, preferred_element_type=jnp.float32)
        low_b = lax.broadcasted_iota(jnp.int32, (BLOCK, qr), 1) < HEAD_DIM
        both = jnp.where(low_b, pltpu.roll(o[:BLOCK], HEAD_DIM, 1), o[BLOCK:])
        mix_a[pl.ds(begin, BLOCK), :] = both.astype(jnp.bfloat16)
        return carry

    lax.fori_loop(0, plane // BLOCK, att_step, 0)

    @pl.when(is_end)
    def _():
        g_copy.wait_recv()

    def group(cc):
        spans = [pl.ds(pl.multiple_of((2 * q + cc) * rows, rows), rows) for q in range(4)]
        return [jnp.concatenate([mix_a[w, :], mix_c[w, :]], axis=1) for w in spans]

    mine_rows = jnp.concatenate(group(c), axis=0)
    other_rows = jnp.concatenate(group(1 - c), axis=0)
    rs_copies = []

    def send_rs(src, dst, stage_id, s, peer):
        copy = remote(src, dst, rs_send.at[stage_id, s], rs_recv.at[stage_id, s], peer)
        copy.start()
        rs_copies.append(copy)

    def stage_a(k):
        source = z if k == 0 else source_of(jnp.int32(k))
        for half in range(2):
            s = 2 * source + half
            if k:
                hop(wout, s, out_up, out_recv, up).wait_recv()
                forward(wout, s, source, out_up, out_down, out_recv)
            weight = wout[s]
            s1[s] = jnp.dot(
                other_rows, weight, preferred_element_type=jnp.float32
            ).astype(jnp.bfloat16).reshape(2, 2, rows, depth)
            send_rs(s1.at[s], r1.at[s], 0, s, c_peer)
            keep[s] = jnp.dot(
                mine_rows, weight, preferred_element_type=jnp.float32
            ).reshape(2, 2, rows, depth)

    def axis_index_of(half):
        return (y, x) if half == 0 else (x, y)

    def stage_b(k):
        source = z if k == 0 else source_of(jnp.int32(k))
        for half in range(2):
            s = 2 * source + half
            remote(s1.at[s], r1.at[s], rs_send.at[0, s], rs_recv.at[0, s], c_peer).wait_recv()
            for j in range(2):
                if half == 0:
                    s2[s, j] = (keep[s, 1 - y, j] + r1[s, 1 - y, j].astype(jnp.float32)).astype(
                        jnp.bfloat16
                    )
                else:
                    s2[s, j] = (keep[s, j, 1 - x] + r1[s, j, 1 - x].astype(jnp.float32)).astype(
                        jnp.bfloat16
                    )
            send_rs(s2.at[s], r2.at[s], 1, s, y_peer if half == 0 else x_peer)

    def stage_c(k):
        source = z if k == 0 else source_of(jnp.int32(k))
        for half in range(2):
            s = 2 * source + half
            peer = y_peer if half == 0 else x_peer
            remote(s2.at[s], r2.at[s], rs_send.at[1, s], rs_recv.at[1, s], peer).wait_recv()
            my = x if half == 0 else y
            for own, j in ((False, 1 - my), (True, my)):
                if half == 0:
                    part = keep[s, y, j] + r1[s, y, j].astype(jnp.float32)
                else:
                    part = keep[s, j, x] + r1[s, j, x].astype(jnp.float32)
                part = part + r2[s, j].astype(jnp.float32)
                if own:
                    keep[s, y, x] = part
                else:
                    s3[s] = part.astype(jnp.bfloat16)
                    send_rs(s3.at[s], r3.at[s], 2, s, x_peer if half == 0 else y_peer)

    def stage_d(k):
        source = z if k == 0 else source_of(jnp.int32(k))
        for half in range(2):
            s = 2 * source + half
            peer = x_peer if half == 0 else y_peer
            remote(s3.at[s], r3.at[s], rs_send.at[2, s], rs_recv.at[2, s], peer).wait_recv()
            out_ref[:, columns(s)] = (keep[s, y, x] + r3[s].astype(jnp.float32)).astype(
                jnp.bfloat16
            )

    for k in range(line):
        stage_a(k)
        if k >= 1:
            stage_c(k - 1)
        stage_b(k)
        if k >= 1:
            stage_d(k - 1)
    stage_c(line - 1)
    stage_d(line - 1)

    for copy in [y_copy, oy_copy] + tok_copies + rs_copies:
        copy.wait_send()

    @pl.when(has_up)
    def _():
        rim_up.wait_send()

    @pl.when(has_down)
    def _():
        rim_down.wait_send()

    @pl.when(is_end)
    def _():
        end_tok(own_block, 0).wait_send()
        end_tok(yb0, 1).wait_send()

    @pl.when(is_help)
    def _():
        for slot in range(2, 8):
            tok2_hop(own_block, slot, x_peer).wait_send()
        g_copy.wait_send()

    @pl.when(from_up)
    def _():
        prod_up.wait_send()

    @pl.when(from_down)
    def _():
        prod_down.wait_send()

    for s in range(2 * line):
        in_sends(s, s // 2, lambda copy: copy.wait_send())

        @pl.when((s // 2 <= z) & has_up)
        def _():
            hop(wout, s, out_up, out_recv, up).wait_send()

        @pl.when((s // 2 >= z) & has_down)
        def _():
            hop(wout, s, out_down, out_recv, down).wait_send()


def trig_table(total):
    half = HEAD_DIM // 2
    freq = np.float64(ROPE_BASE) ** (-np.arange(half) / half)
    angle = np.arange(total)[:, None] * freq
    cosine, sine = np.cos(angle), np.sin(angle)
    return np.concatenate([cosine, cosine, -sine, sine], axis=1).astype(np.float32)


def fused_device(
    tokens, norm_gain, query_weight, key_weight, value_weight, gate_weight, left_weight,
    input_weight, query_gain, key_gain, sink_logit, conv_weight, out_attention, out_conv,
):
    sp_count = lax.axis_size("sp")
    line = sp_count // 2
    rows, width = tokens.shape
    depth = query_weight.shape[1]
    qr = query_weight.shape[0] // 2
    kr = key_weight.shape[0]
    cr = gate_weight.shape[0] // 2
    fan = qr + 2 * kr + 3 * cr
    plane = 8 * rows
    dims = dict(line=line, rows=rows, depth=depth, qr=qr, kr=kr, cr=cr)
    vm = pl.BlockSpec(memory_space=pltpu.VMEM)
    sm = pl.BlockSpec(memory_space=pltpu.SMEM)
    hb = pl.BlockSpec(memory_space=pl.ANY)
    bf16, f32 = jnp.bfloat16, jnp.float32
    dma = pltpu.SemaphoreType.DMA
    n = sp_count
    scratch = [
        pltpu.VMEM((rows, width), bf16),
        pltpu.VMEM((plane, 2 * HEAD_DIM), f32),
        pltpu.VMEM((fan, depth), bf16),
        pltpu.VMEM((qr + cr, depth), bf16),
        pltpu.VMEM((n, fan, depth), bf16),
        pltpu.VMEM((n, qr + cr, depth), bf16),
        pltpu.VMEM((8, rows, width), bf16),
        pltpu.VMEM((8, rows, width), bf16),
        pltpu.VMEM((plane, fan), f32),
        pltpu.VMEM((plane, 3 * cr), f32),
        pltpu.VMEM((plane + 2 * WINDOW, qr), bf16),
        pltpu.VMEM((plane + 32, cr), bf16),
        pltpu.VMEM((plane + 32, cr), bf16),
        pltpu.VMEM((plane, qr), bf16),
        pltpu.VMEM((plane, cr), bf16),
        pltpu.VMEM((plane, cr), bf16),
        pltpu.VMEM((2, plane, qr), bf16),
        pltpu.VMEM((n, 2, 2, rows, depth), f32),
        pltpu.VMEM((n, 2, 2, rows, depth), bf16),
        pltpu.VMEM((n, 2, 2, rows, depth), bf16),
        pltpu.VMEM((n, 2, rows, depth), bf16),
        pltpu.VMEM((n, 2, rows, depth), bf16),
        pltpu.VMEM((n, rows, depth), bf16),
        pltpu.VMEM((n, rows, depth), bf16),
        dma((18,)), dma((1,)), dma((1,)), dma((n,)), dma((n,)),
        dma((n,)), dma((n,)), dma((n,)), dma((n,)),
        dma((7,)), dma((8,)), dma((8,)), dma((8,)), dma((2,)), dma((2,)), dma((2,)), dma((2,)),
        dma((1,)), dma((1,)), dma((3, n)), dma((3, n)),
    ]
    taps = conv_weight.reshape(3, 2, cr).transpose(1, 0, 2)
    return pl.pallas_call(
        functools.partial(fused_kernel, dims),
        out_shape=jax.ShapeDtypeStruct((rows, width), bf16),
        in_specs=[hb, vm, hb, hb, hb, hb, hb, hb, vm, vm, sm, vm, hb, hb, hb],
        out_specs=vm,
        scratch_shapes=scratch,
        compiler_params=pltpu.CompilerParams(
            collective_id=0, has_side_effects=True, vmem_limit_bytes=56 * 1024 * 1024
        ),
    )(
        tokens, norm_gain[None, :], query_weight, key_weight, value_weight, gate_weight,
        left_weight, input_weight, query_gain[None, :],
        key_gain[None, :], sink_logit[None, :], taps, out_attention, out_conv,
        jnp.asarray(trig_table(plane * line)),
    )


def local_device(*args):
    tokens, query_weight, key_weight, gate_weight = args[0], args[2], args[3], args[5]
    fits = (
        lax.axis_size("sp") % 2 == 0
        and 8 <= lax.axis_size("sp") <= 16
        and lax.axis_size("tp") == 4
        and query_weight.shape[1] % 128 == 0
        and query_weight.shape[0] == 4 * HEAD_DIM
        and key_weight.shape[0] == HEAD_DIM
        and gate_weight.shape[0] == 256
        and tokens.shape[0] % 16 == 0
        and 8 * tokens.shape[0] % BLOCK == 0
    )
    return fused_device(*args) if fits else per_device(*args)


def solution(mesh):
    in_specs = (
        P(("sp", "tp"), None),
        P(),
        P("tp", "sp"),
        P("tp", "sp"),
        P("tp", "sp"),
        P("tp", "sp"),
        P("tp", "sp"),
        P("tp", "sp"),
        P(),
        P(),
        P("tp"),
        P(None, "tp"),
        P("tp", "sp"),
        P("tp", "sp"),
    )
    out_specs = P(("sp", "tp"), None)
    return jax.shard_map(
        local_device, mesh=mesh, in_specs=in_specs, out_specs=out_specs, check_vma=False
    )
```

```python
import functools

import jax
import jax.numpy as jnp
import numpy as np
from jax import lax
from jax.experimental import pallas as pl
from jax.experimental.pallas import tpu as pltpu
from jax.sharding import PartitionSpec as P

HEAD_DIM = 64
WINDOW = 128
BLOCK = 128


EPS = 1e-06
ROPE_BASE = 10000.0
NEG_FILL = -1e30


def with_halo(cells, sides, width):
    for axis, dim in sides:
        count = lax.axis_size(axis)
        ends = count - 1
        head = lax.slice_in_dim(cells, 0, width, axis=dim)
        tail = lax.slice_in_dim(cells, cells.shape[dim] - width, cells.shape[dim], axis=dim)
        cells = jnp.concatenate(
            [
                lax.ppermute(tail, axis, [(i, (i + 1) % count) for i in range(ends)]),
                cells,
                lax.ppermute(head, axis, [((i + 1) % count, i) for i in range(ends)]),
            ],
            axis=dim,
        )
    return cells


def normalize(values, gain):
    return values * lax.rsqrt(jnp.mean(values * values, axis=-1, keepdims=True) + EPS) * gain


def rotate(values, positions):
    half = values.shape[-1] // 2
    freq = ROPE_BASE ** (-jnp.arange(half, dtype=jnp.float32) / half)
    angle = positions[:, None] * freq
    cosine = jnp.cos(angle)[:, None, :]
    sine = jnp.sin(angle)[:, None, :]
    first = values[..., :half]
    second = values[..., half:]
    return jnp.concatenate(
        [first * cosine - second * sine, second * cosine + first * sine], axis=-1
    )


def project(rows, weight):
    return lax.dot_general(
        rows, weight, (((1,), (1,)), ((), ())), preferred_element_type=jnp.float32
    ).astype(jnp.bfloat16)


def attend(query_rot, key_rim, value_rim, sinks, offset, total):
    count = query_rot.shape[0]
    local_heads = query_rot.shape[1]
    kv_local = key_rim.shape[1]
    group = local_heads // kv_local
    span = BLOCK + 2 * WINDOW
    nblocks = count // BLOCK
    shaped = query_rot.reshape(nblocks, BLOCK, kv_local, group, HEAD_DIM)
    sink_group = sinks.reshape(kv_local, group)[:, :, None]

    def one_block(packed):
        block_index, query_block = packed
        begin = block_index * BLOCK
        key_block = lax.dynamic_slice_in_dim(key_rim, begin, span, 0)
        value_block = lax.dynamic_slice_in_dim(value_rim, begin, span, 0)
        scores = jnp.einsum(
            "qkgd,nkd->kgqn", query_block, key_block, preferred_element_type=jnp.float32
        ) * HEAD_DIM ** (-0.5)
        query_pos = offset + begin + jnp.arange(BLOCK, dtype=jnp.int32)
        key_pos = offset + begin - WINDOW + jnp.arange(span, dtype=jnp.int32)
        allowed = (
            (jnp.abs(query_pos[:, None] - key_pos[None, :]) <= WINDOW)
            & (key_pos >= 0)[None, :]
            & (key_pos < total)[None, :]
        )
        scores = jnp.where(allowed, scores, NEG_FILL)
        top = jnp.maximum(jnp.max(scores, axis=-1), sink_group)
        expo = jnp.exp(scores - top[..., None])
        denom = jnp.sum(expo, axis=-1) + jnp.exp(sink_group - top)
        weights = (expo / denom[..., None]).astype(jnp.bfloat16)
        return jnp.einsum(
            "kgqn,nkd->qkgd", weights, value_block, preferred_element_type=jnp.float32
        ).astype(jnp.bfloat16)

    result = lax.map(one_block, (jnp.arange(nblocks, dtype=jnp.int32), shaped))
    return result.reshape(count, local_heads * HEAD_DIM)


def per_device(
    tokens,
    norm_gain,
    query_weight,
    key_weight,
    value_weight,
    gate_weight,
    left_weight,
    input_weight,
    query_gain,
    key_gain,
    sink_logit,
    conv_weight,
    out_attention,
    out_conv,
):
    sp_count = lax.axis_size("sp")
    sp_place = lax.axis_index("sp")
    gathered = (
        lax.all_gather(query_weight, "sp", axis=1, tiled=True),
        lax.all_gather(key_weight, "sp", axis=1, tiled=True),
        lax.all_gather(value_weight, "sp", axis=1, tiled=True),
        lax.all_gather(gate_weight, "sp", axis=1, tiled=True),
        lax.all_gather(left_weight, "sp", axis=1, tiled=True),
        lax.all_gather(input_weight, "sp", axis=1, tiled=True),
        lax.all_gather(out_attention, "sp", axis=1, tiled=True),
        lax.all_gather(out_conv, "sp", axis=1, tiled=True),
    )
    (
        query_full,
        key_full,
        value_full,
        gate_full,
        left_full,
        input_full,
        attn_out_full,
        conv_out_full,
    ) = gathered
    normed = normalize(tokens.astype(jnp.float32), norm_gain).astype(jnp.bfloat16)
    widths = [
        query_full.shape[0],
        key_full.shape[0],
        value_full.shape[0],
        gate_full.shape[0],
        left_full.shape[0],
        input_full.shape[0],
    ]
    piece = lax.all_gather(normed, "tp", axis=0, tiled=True)
    joined = jnp.concatenate(
        [
            project(piece, weight)
            for weight in (query_full, key_full, value_full, gate_full, left_full, input_full)
        ],
        axis=1,
    )
    count = joined.shape[0]
    bounds = [0]
    for width in widths:
        bounds.append(bounds[-1] + width)
    query, keys, values, gate, left, inputs = [
        joined[:, bounds[place] : bounds[place + 1]] for place in range(6)
    ]
    offset = sp_place * count
    total = count * sp_count
    positions = (offset + jnp.arange(count, dtype=jnp.int32)).astype(jnp.float32)
    local_heads = widths[0] // HEAD_DIM
    kv_local = widths[1] // HEAD_DIM
    query_rot = rotate(
        normalize(query.reshape(count, local_heads, HEAD_DIM).astype(jnp.float32), query_gain),
        positions,
    ).astype(jnp.bfloat16)
    key_rot = rotate(
        normalize(keys.reshape(count, kv_local, HEAD_DIM).astype(jnp.float32), key_gain), positions
    ).astype(jnp.bfloat16)
    key_flat = key_rot.reshape(count, kv_local * HEAD_DIM)
    product = (left.astype(jnp.float32) * inputs.astype(jnp.float32)).astype(jnp.bfloat16)
    kv_width = widths[1]
    pair_rim = with_halo(jnp.concatenate([key_flat, values], axis=1), (("sp", 0),), WINDOW)
    product_rim = with_halo(product, (("sp", 0),), 1)
    rim_rows = pair_rim.shape[0]
    key_rim = pair_rim[:, :kv_width].reshape(rim_rows, kv_local, HEAD_DIM)
    value_rim = pair_rim[:, kv_width:].reshape(rim_rows, kv_local, HEAD_DIM)
    attended = attend(query_rot, key_rim, value_rim, sink_logit, offset, total)
    padded = product_rim.astype(jnp.float32)
    convolved = (
        conv_weight[0] * padded[:-2] + conv_weight[1] * padded[1:-1] + conv_weight[2] * padded[2:]
    )
    gated = (gate.astype(jnp.float32) * convolved).astype(jnp.bfloat16)
    return lax.psum_scatter(
        (
            jnp.dot(attended, attn_out_full, preferred_element_type=jnp.float32)
            + jnp.dot(gated, conv_out_full, preferred_element_type=jnp.float32)
        ).astype(jnp.bfloat16),
        "tp",
        scatter_dimension=0,
        tiled=True,
    )


MESH = pl.DeviceIdType.MESH


def fused_kernel(
    dims,
    tok_hbm, gain_ref, q_hbm, k_hbm, v_hbm, g_hbm, l_hbm, i_hbm,
    qgain_ref, kgain_ref, sink_ref, conv_ref, oa_hbm, oc_hbm, trig_hbm,
    out_ref,
    tok, trig, stage, ostage, win, wout, normed, normed2, acc, acc2, rim, prod, prod2, mix_a, mix_c, gated2,
    qrot,
    keep, s1, r1, s2, r2, s3, r3,
    local_sem, y_send, oy_send, in_recv, out_recv, in_up, in_down, out_up, out_down,
    tok_send, tok_recv, tok2_send, tok2_recv, rim_send, rim_recv, prod_send, prod_recv, g_send, g_recv,
    rs_send, rs_recv,
):
    line, rows, depth, qr, kr, cr = (
        dims["line"], dims["rows"], dims["depth"], dims["qr"], dims["kr"], dims["cr"]
    )
    sp = lax.axis_index("sp")
    tp = lax.axis_index("tp")
    z, y = sp // 2, sp % 2
    x, c = tp // 2, tp % 2
    y_peer = (2 * z + 1 - y, tp)
    x_peer = (sp, 2 * (1 - x) + c)
    c_peer = (sp, 2 * x + 1 - c)
    up = (jnp.minimum(2 * (z + 1) + y, 2 * line - 1), tp)
    down = (jnp.maximum(2 * (z - 1) + y, 0), tp)
    has_up = z < line - 1
    has_down = z > 0
    s_own = sp
    s_mate = 2 * z + 1 - y
    plane = 8 * rows
    core = qr + 2 * kr
    is_end = (z == 0) | (z == line - 1)
    not_end = (z > 0) & (z < line - 1)
    is_help = (z == 1) | (z == line - 2)
    help_dev = (jnp.where(z == 0, 2 + y, 2 * (line - 2) + y), tp)
    end_dev = (jnp.where(z == 1, y, 2 * (line - 1) + y), tp)

    barrier = pltpu.get_barrier_semaphore()
    for peer in (y_peer, x_peer, c_peer):
        pl.semaphore_signal(barrier, inc=1, device_id=peer, device_id_type=MESH)

    @pl.when(has_up)
    def _():
        pl.semaphore_signal(barrier, inc=1, device_id=up, device_id_type=MESH)

    @pl.when(has_down)
    def _():
        pl.semaphore_signal(barrier, inc=1, device_id=down, device_id_type=MESH)

    counter = [0]

    def local(src, dst):
        copy = pltpu.make_async_copy(src, dst, local_sem.at[counter[0]])
        counter[0] += 1
        copy.start()
        return copy

    def pieces(which, dst):
        q0, c0 = pl.multiple_of(which * qr, qr), pl.multiple_of(which * cr, cr)
        return [
            local(q_hbm.at[pl.ds(q0, qr)], dst.at[0:qr]),
            local(k_hbm, dst.at[qr : qr + kr]),
            local(v_hbm, dst.at[qr + kr : qr + 2 * kr]),
            local(g_hbm.at[pl.ds(c0, cr)], dst.at[qr + 2 * kr : qr + 2 * kr + cr]),
            local(l_hbm.at[pl.ds(c0, cr)], dst.at[qr + 2 * kr + cr : qr + 2 * kr + 2 * cr]),
            local(i_hbm.at[pl.ds(c0, cr)], dst.at[qr + 2 * kr + 2 * cr : qr + 2 * kr + 3 * cr]),
        ]

    def out_pieces(which, dst):
        q0, c0 = pl.multiple_of(which * qr, qr), pl.multiple_of(which * cr, cr)
        return [
            local(oa_hbm.at[pl.ds(q0, qr)], dst.at[0:qr]),
            local(oc_hbm.at[pl.ds(c0, cr)], dst.at[qr : qr + cr]),
        ]

    mine = pieces(y, win.at[s_own])
    theirs = pieces(1 - y, stage)
    tok_copy = local(tok_hbm, tok)
    out_theirs = out_pieces(1 - y, ostage)
    out_mine = out_pieces(y, wout.at[s_own])
    trig_copy = local(trig_hbm.at[pl.ds(pl.multiple_of(z * plane, plane), plane)], trig)

    pl.semaphore_wait(barrier, 3 + has_up.astype(jnp.int32) + has_down.astype(jnp.int32))

    def remote(src, dst, send, recv, peer):
        return pltpu.make_async_remote_copy(
            src_ref=src, dst_ref=dst, send_sem=send, recv_sem=recv,
            device_id=peer, device_id_type=MESH,
        )

    def hop(buf, s, send, recv, peer):
        return remote(buf.at[s], buf.at[s], send.at[s], recv.at[s], peer)

    chunks = ((0, core), (core, core + 3 * cr))

    def in_hop(s, part, send, peer):
        lo, hi = chunks[part]
        return remote(
            win.at[s, lo:hi], win.at[s, lo:hi], send.at[part, s], in_recv.at[part, s], peer
        )

    def in_sends(s, source, part, act):
        for inner, edge, way, send, peer in (
            (z + 1 < line - 1, has_up, source <= z, in_up, up),
            (z - 1 > 0, has_down, source >= z, in_down, down),
        ):
            @pl.when(way & (edge if part == 0 else inner))
            def _():
                act(in_hop(s, part, send, peer))

    def in_forward(s, source, part):
        in_sends(s, source, part, lambda copy: copy.start())

    up_full = z + 1 < line - 1
    down_full = z - 1 > 0

    def forward(buf, s, source, ups, downs, recv):
        @pl.when((source <= z) & has_up)
        def _():
            hop(buf, s, ups, recv, up).start()

        @pl.when((source >= z) & has_down)
        def _():
            hop(buf, s, downs, recv, down).start()

    for copy in mine:
        copy.wait()
    for part in range(2):
        in_forward(s_own, z, part)
    for copy in theirs:
        copy.wait()
    y_copies = [
        remote(
            stage.at[lo:hi], win.at[s_own, lo:hi], y_send.at[part], in_recv.at[part, s_own], y_peer
        )
        for part, (lo, hi) in enumerate(chunks)
    ]
    for copy in y_copies:
        copy.start()
    tok_copy.wait()
    t = tok[...].astype(jnp.float32)
    t = t * lax.rsqrt(jnp.mean(t * t, axis=-1, keepdims=True) + EPS) * gain_ref[...]
    own_block = 4 * y + 2 * x + c
    normed[own_block] = t.astype(jnp.bfloat16)

    def end_tok(block, slot):
        return remote(
            normed.at[block], normed2.at[block], tok2_send.at[slot], tok2_recv.at[block], help_dev
        )

    def tok2_hop(block, slot, peer):
        return remote(
            normed2.at[block], normed2.at[block], tok2_send.at[slot], tok2_recv.at[block], peer
        )

    for copy in out_theirs:
        copy.wait()
    oy_copy = remote(ostage, wout.at[s_own], oy_send.at[0], out_recv.at[s_own], y_peer)
    oy_copy.start()
    for copy in out_mine:
        copy.wait()

    @pl.when(is_end)
    def _():
        end_tok(own_block, 0).start()

    def block_of(yy, xx, cc):
        return 4 * yy + 2 * xx + cc

    def tok_hop(block, slot, peer):
        return remote(
            normed.at[block], normed.at[block], tok_send.at[slot], tok_recv.at[block], peer
        )

    xb = block_of(y, 1 - x, c)
    yb0 = block_of(1 - y, x, c)
    yb1 = block_of(1 - y, 1 - x, c)
    tok_copies = [
        tok_hop(own_block, 0, x_peer),
        tok_hop(own_block, 1, y_peer),
        tok_hop(own_block, 2, c_peer),
    ]
    for copy in tok_copies:
        copy.start()

    for part in range(2):
        in_hop(s_mate, part, in_up, up).wait_recv()
        in_forward(s_mate, z, part)

    def tok_wait(block):
        tok_hop(block, 0, x_peer).wait_recv()

    tok_wait(xb)
    more = [tok_hop(xb, 3, y_peer), tok_hop(xb, 4, c_peer)]
    for copy in more:
        copy.start()
    tok_copies += more

    hop(wout, s_mate, out_up, out_recv, up).wait_recv()

    def own_out(flag_up, flag_down):
        for s in (s_own, s_mate):
            @pl.when(flag_up & has_up)
            def _():
                hop(wout, s, out_up, out_recv, up).start()

            @pl.when(flag_down & has_down)
            def _():
                hop(wout, s, out_down, out_recv, down).start()

    tok_wait(yb0)

    @pl.when(is_end)
    def _():
        end_tok(yb0, 1).start()

    own_out(z == 0, z == line - 1)
    copy = tok_hop(yb0, 5, c_peer)
    copy.start()
    tok_copies.append(copy)
    tok_wait(yb1)
    copy = tok_hop(yb1, 6, c_peer)
    copy.start()
    tok_copies.append(copy)
    for yy in range(2):
        for xx in range(2):
            tok_wait(block_of(yy, xx, 1 - c))

    def columns(s):
        return pl.ds(pl.multiple_of(s * depth, depth), depth)

    def dot_t(a, w):
        return lax.dot_general(a, w, (((1,), (1,)), ((), ())), preferred_element_type=jnp.float32)

    def in_dot(s, first):
        a = normed[:, :, columns(s)].reshape(plane, depth)
        low_part = dot_t(a, win[s, 0:core])
        acc[:, 0:core] = low_part if first else acc[:, 0:core] + low_part

        @pl.when(not_end)
        def _():
            high_part = dot_t(a, win[s, core:])
            acc[:, core:] = high_part if first else acc[:, core:] + high_part

    paired = jnp.minimum(z, line - 1 - z)
    below_longer = z > line - 1 - z

    def source_of(k):
        d = jnp.where(k <= 2 * paired, (k + 1) // 2, k - paired)
        below = jnp.where(k <= 2 * paired, k % 2 == 1, below_longer)
        return jnp.where(below, z - d, z + d)

    in_dot(s_own, True)
    in_dot(s_mate, False)

    def in_step(k, carry):
        source = source_of(k)
        for turn, block, slot in ((2, own_block, 2), (line - 1, yb0, 4)):
            @pl.when(is_help & (k == turn))
            def _():
                tok2_hop(block, slot, end_dev).wait_recv()
                tok2_hop(block, slot, x_peer).start()
                tok2_hop(block, slot + 1, c_peer).start()

        for half in range(2):
            first = jnp.where(half == 0, y, 1 - y)
            s = 2 * source + first
            in_hop(s, 0, in_up, up).wait_recv()
            in_forward(s, source, 0)

            @pl.when(not_end)
            def _():
                in_hop(s, 1, in_up, up).wait_recv()
                in_forward(s, source, 1)

            if half == 1:
                own_out(source == 0, source == line - 1)
            in_dot(s, False)
        return carry

    lax.fori_loop(1, line, in_step, 0)

    trig_copy.wait()
    lane = lax.broadcasted_iota(jnp.int32, (plane, qr), 1)
    half_dim = HEAD_DIM // 2
    table = trig[...]
    cos2 = jnp.where(lane < HEAD_DIM, table, pltpu.roll(table, HEAD_DIM, 1))
    sin2 = jnp.where(lane < HEAD_DIM, pltpu.roll(table, HEAD_DIM, 1), table)
    low = lane < HEAD_DIM
    first_half = lane % HEAD_DIM < half_dim

    def rot(v):
        partner = jnp.where(
            first_half, pltpu.roll(v, qr - half_dim, 1), pltpu.roll(v, half_dim, 1)
        )
        return v * cos2 + partner * sin2

    def bf(v):
        return v.astype(jnp.bfloat16).astype(jnp.float32)

    kv = bf(acc[:, qr : 2 * qr])
    ksq = jnp.sum(jnp.where(low, kv * kv, 0.0), axis=-1, keepdims=True) / HEAD_DIM
    kgain = jnp.concatenate([kgain_ref[...], kgain_ref[...]], axis=1)
    kn = kv * lax.rsqrt(ksq + EPS) * kgain
    krot = rot(kn)
    rim[WINDOW : WINDOW + plane, :] = jnp.where(low, krot, kv).astype(jnp.bfloat16)
    base = 2 * qr

    qv = bf(acc[:, 0:qr])
    qq = qv * qv
    q_lo = jnp.sum(jnp.where(low, qq, 0.0), axis=-1, keepdims=True) / HEAD_DIM
    q_hi = jnp.sum(jnp.where(low, 0.0, qq), axis=-1, keepdims=True) / HEAD_DIM
    qgain = jnp.concatenate([qgain_ref[...], qgain_ref[...]], axis=1)
    qn = qv * lax.rsqrt(jnp.where(low, q_lo, q_hi) + EPS) * qgain
    qro = rot(qn)

    bottom = pl.ds(WINDOW, WINDOW)
    top = pl.ds(plane, WINDOW)
    rim_up = remote(rim.at[top], rim.at[pl.ds(0, WINDOW)], rim_send.at[0], rim_recv.at[0], up)
    rim_down = remote(
        rim.at[bottom], rim.at[pl.ds(WINDOW + plane, WINDOW)], rim_send.at[1], rim_recv.at[1], down
    )

    @pl.when(has_up)
    def _():
        rim_up.start()

    @pl.when(has_down)
    def _():
        rim_down.start()

    zero_rim = jnp.zeros((WINDOW, qr), jnp.bfloat16)

    @pl.when(z == 0)
    def _():
        rim[0:WINDOW] = zero_rim

    @pl.when(z == line - 1)
    def _():
        rim[WINDOW + plane :] = zero_rim

    qrot[0] = jnp.where(low, qro, 0.0).astype(jnp.bfloat16)
    qrot[1] = jnp.where(low, pltpu.roll(qro, HEAD_DIM, 1), 0.0).astype(jnp.bfloat16)

    pad = 16
    zero_pad = jnp.zeros((pad, cr), jnp.bfloat16)
    taps = conv_ref[y]

    def convolve(ref, gate):
        p = ref[...].astype(jnp.float32)
        before = pltpu.roll(p, 1, 0)[pad : pad + plane]
        after = pltpu.roll(p, plane + 2 * pad - 1, 0)[pad : pad + plane]
        mixed = taps[0:1] * before + taps[1:2] * p[pad : pad + plane] + taps[2:3] * after
        return (gate * mixed).astype(jnp.bfloat16)

    prod_up = remote(
        prod.at[pl.ds(plane, pad)], prod.at[pl.ds(0, pad)], prod_send.at[0], prod_recv.at[0], up
    )
    prod_down = remote(
        prod.at[pl.ds(pad, pad)], prod.at[pl.ds(pad + plane, pad)],
        prod_send.at[1], prod_recv.at[1], down,
    )
    from_up = not_end & up_full
    from_down = not_end & down_full

    @pl.when(not_end)
    def _():
        left = bf(acc[:, base + cr : base + 2 * cr])
        inputs = bf(acc[:, base + 2 * cr : base + 3 * cr])
        prod[pad : pad + plane] = (left * inputs).astype(jnp.bfloat16)

    @pl.when(from_up)
    def _():
        prod_up.start()

    @pl.when(from_down)
    def _():
        prod_down.start()

    def out_take(k):
        source = source_of(jnp.int32(k))
        for half in range(2):
            s = 2 * source + half
            hop(wout, s, out_up, out_recv, up).wait_recv()
            forward(wout, s, source, out_up, out_down, out_recv)

    def inner_take(k):
        @pl.when(not_end)
        def _():
            out_take(k)

    inner_take(1)
    g_copy = remote(gated2, mix_c, g_send.at[0], g_recv.at[0], end_dev)

    @pl.when(is_help)
    def _():
        for block, slot in ((xb, 6), (yb1, 7)):
            tok2_hop(block, slot, x_peer).wait_recv()
            tok2_hop(block, slot, c_peer).start()
        for yy in range(2):
            for xx in range(2):
                tok2_hop(block_of(yy, xx, 1 - c), 0, c_peer).wait_recv()
        acc2[...] = jnp.zeros_like(acc2)

        def help_step(s, carry):
            a = normed2[:, :, columns(s)].reshape(plane, depth)
            acc2[...] += dot_t(a, win[s, core:])
            return carry

        lax.fori_loop(0, 2 * line, help_step, 0)
        prod2[pad : pad + plane] = (
            bf(acc2[:, cr : 2 * cr]) * bf(acc2[:, 2 * cr : 3 * cr])
        ).astype(jnp.bfloat16)

        @pl.when(z == 1)
        def _():
            prod2[0:pad] = zero_pad
            prod2[pad + plane :] = prod[pad : 2 * pad]
            prod[0:pad] = prod2[plane : plane + pad]

        @pl.when(z != 1)
        def _():
            prod2[0:pad] = prod[plane : plane + pad]
            prod2[pad + plane :] = zero_pad
            prod[pad + plane :] = prod2[pad : 2 * pad]

        gated2[...] = convolve(prod2, bf(acc2[:, 0:cr]))
        g_copy.start()

    @pl.when(from_up)
    def _():
        prod_down.wait_recv()

    @pl.when(from_down)
    def _():
        prod_up.wait_recv()

    @pl.when(not_end)
    def _():
        mix_c[...] = convolve(prod, bf(acc[:, base : base + cr]))

    for k in range(2, line - 1):
        inner_take(k)

    @pl.when(has_down)
    def _():
        rim_up.wait_recv()

    @pl.when(has_up)
    def _():
        rim_down.wait_recv()

    span = BLOCK + 2 * WINDOW
    total = plane * line

    def att_step(block, carry):
        begin = pl.multiple_of(block * BLOCK, BLOCK)
        kvb = rim[pl.ds(begin, span), :]
        qb = qrot[:, pl.ds(begin, BLOCK), :].reshape(2 * BLOCK, qr)
        scores = lax.dot_general(
            qb, kvb, (((1,), (1,)), ((), ())), preferred_element_type=jnp.float32
        ) * HEAD_DIM ** (-0.5)
        row = lax.broadcasted_iota(jnp.int32, (2 * BLOCK, span), 0)
        col = lax.broadcasted_iota(jnp.int32, (2 * BLOCK, span), 1)
        gap = row % BLOCK + WINDOW - col
        pos = z * plane + begin - WINDOW + col
        allowed = (gap <= WINDOW) & (gap >= -WINDOW) & (pos >= 0) & (pos < total)
        scores = jnp.where(allowed, scores, NEG_FILL)
        head = lax.broadcasted_iota(jnp.int32, (2 * BLOCK, 1), 0)
        sink = jnp.where(head < BLOCK, sink_ref[0, 2 * y], sink_ref[0, 2 * y + 1])
        peak = jnp.maximum(jnp.max(scores, axis=-1, keepdims=True), sink)
        expo = jnp.exp(scores - peak)
        denom = jnp.sum(expo, axis=-1, keepdims=True) + jnp.exp(sink - peak)
        weights = (expo / denom).astype(jnp.bfloat16)
        o = jnp.dot(weights, kvb, preferred_element_type=jnp.float32)
        low_b = lax.broadcasted_iota(jnp.int32, (BLOCK, qr), 1) < HEAD_DIM
        both = jnp.where(low_b, pltpu.roll(o[:BLOCK], HEAD_DIM, 1), o[BLOCK:])
        mix_a[pl.ds(begin, BLOCK), :] = both.astype(jnp.bfloat16)
        return carry

    lax.fori_loop(0, plane // BLOCK, att_step, 0)

    @pl.when(is_end)
    def _():
        g_copy.wait_recv()

    def group(cc):
        spans = [pl.ds(pl.multiple_of((2 * q + cc) * rows, rows), rows) for q in range(4)]
        return [jnp.concatenate([mix_a[w, :], mix_c[w, :]], axis=1) for w in spans]

    mine_rows = jnp.concatenate(group(c), axis=0)
    other_rows = jnp.concatenate(group(1 - c), axis=0)
    rs_copies = []

    def send_rs(src, dst, stage_id, s, peer):
        copy = remote(src, dst, rs_send.at[stage_id, s], rs_recv.at[stage_id, s], peer)
        copy.start()
        rs_copies.append(copy)

    def stage_a(k):
        source = z if k == 0 else source_of(jnp.int32(k))
        if k:
            @pl.when(is_end)
            def _():
                out_take(k)

        for half in range(2):
            s = 2 * source + half
            weight = wout[s]
            s1[s] = jnp.dot(
                other_rows, weight, preferred_element_type=jnp.float32
            ).astype(jnp.bfloat16).reshape(2, 2, rows, depth)
            send_rs(s1.at[s], r1.at[s], 0, s, c_peer)
            keep[s] = jnp.dot(
                mine_rows, weight, preferred_element_type=jnp.float32
            ).reshape(2, 2, rows, depth)

    def axis_index_of(half):
        return (y, x) if half == 0 else (x, y)

    def stage_b(k):
        source = z if k == 0 else source_of(jnp.int32(k))
        for half in range(2):
            s = 2 * source + half
            remote(s1.at[s], r1.at[s], rs_send.at[0, s], rs_recv.at[0, s], c_peer).wait_recv()
            for j in range(2):
                if half == 0:
                    s2[s, j] = (keep[s, 1 - y, j] + r1[s, 1 - y, j].astype(jnp.float32)).astype(
                        jnp.bfloat16
                    )
                else:
                    s2[s, j] = (keep[s, j, 1 - x] + r1[s, j, 1 - x].astype(jnp.float32)).astype(
                        jnp.bfloat16
                    )
            send_rs(s2.at[s], r2.at[s], 1, s, y_peer if half == 0 else x_peer)

    def stage_c(k):
        source = z if k == 0 else source_of(jnp.int32(k))
        for half in range(2):
            s = 2 * source + half
            peer = y_peer if half == 0 else x_peer
            remote(s2.at[s], r2.at[s], rs_send.at[1, s], rs_recv.at[1, s], peer).wait_recv()
            my = x if half == 0 else y
            for own, j in ((False, 1 - my), (True, my)):
                if half == 0:
                    part = keep[s, y, j] + r1[s, y, j].astype(jnp.float32)
                else:
                    part = keep[s, j, x] + r1[s, j, x].astype(jnp.float32)
                part = part + r2[s, j].astype(jnp.float32)
                if own:
                    keep[s, y, x] = part
                else:
                    s3[s] = part.astype(jnp.bfloat16)
                    send_rs(s3.at[s], r3.at[s], 2, s, x_peer if half == 0 else y_peer)

    def stage_d(k):
        source = z if k == 0 else source_of(jnp.int32(k))
        for half in range(2):
            s = 2 * source + half
            peer = x_peer if half == 0 else y_peer
            remote(s3.at[s], r3.at[s], rs_send.at[2, s], rs_recv.at[2, s], peer).wait_recv()
            out_ref[:, columns(s)] = (keep[s, y, x] + r3[s].astype(jnp.float32)).astype(
                jnp.bfloat16
            )

    for k in range(line + 3):
        if k == line - 1:
            inner_take(k)
        for late, step in enumerate((stage_a, stage_b, stage_c, stage_d)):
            if 0 <= k - late < line:
                step(k - late)

    for copy in y_copies + [oy_copy] + tok_copies + rs_copies:
        copy.wait_send()

    @pl.when(has_up)
    def _():
        rim_up.wait_send()

    @pl.when(has_down)
    def _():
        rim_down.wait_send()

    @pl.when(is_end)
    def _():
        end_tok(own_block, 0).wait_send()
        end_tok(yb0, 1).wait_send()

    @pl.when(is_help)
    def _():
        for slot in range(2, 8):
            tok2_hop(own_block, slot, x_peer).wait_send()
        g_copy.wait_send()

    @pl.when(from_up)
    def _():
        prod_up.wait_send()

    @pl.when(from_down)
    def _():
        prod_down.wait_send()

    for s in range(2 * line):
        for part in range(2):
            in_sends(s, s // 2, part, lambda copy: copy.wait_send())

        @pl.when((s // 2 <= z) & has_up)
        def _():
            hop(wout, s, out_up, out_recv, up).wait_send()

        @pl.when((s // 2 >= z) & has_down)
        def _():
            hop(wout, s, out_down, out_recv, down).wait_send()


def trig_table(total):
    half = HEAD_DIM // 2
    freq = np.float64(ROPE_BASE) ** (-np.arange(half) / half)
    angle = np.arange(total)[:, None] * freq
    cosine, sine = np.cos(angle), np.sin(angle)
    return np.concatenate([cosine, cosine, -sine, sine], axis=1).astype(np.float32)


def fused_device(
    tokens, norm_gain, query_weight, key_weight, value_weight, gate_weight, left_weight,
    input_weight, query_gain, key_gain, sink_logit, conv_weight, out_attention, out_conv,
):
    sp_count = lax.axis_size("sp")
    line = sp_count // 2
    rows, width = tokens.shape
    depth = query_weight.shape[1]
    qr = query_weight.shape[0] // 2
    kr = key_weight.shape[0]
    cr = gate_weight.shape[0] // 2
    fan = qr + 2 * kr + 3 * cr
    plane = 8 * rows
    dims = dict(line=line, rows=rows, depth=depth, qr=qr, kr=kr, cr=cr)
    vm = pl.BlockSpec(memory_space=pltpu.VMEM)
    sm = pl.BlockSpec(memory_space=pltpu.SMEM)
    hb = pl.BlockSpec(memory_space=pl.ANY)
    bf16, f32 = jnp.bfloat16, jnp.float32
    dma = pltpu.SemaphoreType.DMA
    n = sp_count
    scratch = [
        pltpu.VMEM((rows, width), bf16),
        pltpu.VMEM((plane, 2 * HEAD_DIM), f32),
        pltpu.VMEM((fan, depth), bf16),
        pltpu.VMEM((qr + cr, depth), bf16),
        pltpu.VMEM((n, fan, depth), bf16),
        pltpu.VMEM((n, qr + cr, depth), bf16),
        pltpu.VMEM((8, rows, width), bf16),
        pltpu.VMEM((8, rows, width), bf16),
        pltpu.VMEM((plane, fan), f32),
        pltpu.VMEM((plane, 3 * cr), f32),
        pltpu.VMEM((plane + 2 * WINDOW, qr), bf16),
        pltpu.VMEM((plane + 32, cr), bf16),
        pltpu.VMEM((plane + 32, cr), bf16),
        pltpu.VMEM((plane, qr), bf16),
        pltpu.VMEM((plane, cr), bf16),
        pltpu.VMEM((plane, cr), bf16),
        pltpu.VMEM((2, plane, qr), bf16),
        pltpu.VMEM((n, 2, 2, rows, depth), f32),
        pltpu.VMEM((n, 2, 2, rows, depth), bf16),
        pltpu.VMEM((n, 2, 2, rows, depth), bf16),
        pltpu.VMEM((n, 2, rows, depth), bf16),
        pltpu.VMEM((n, 2, rows, depth), bf16),
        pltpu.VMEM((n, rows, depth), bf16),
        pltpu.VMEM((n, rows, depth), bf16),
        dma((18,)), dma((2,)), dma((1,)), dma((2, n)), dma((n,)),
        dma((2, n)), dma((2, n)), dma((n,)), dma((n,)),
        dma((7,)), dma((8,)), dma((8,)), dma((8,)), dma((2,)), dma((2,)), dma((2,)), dma((2,)),
        dma((1,)), dma((1,)), dma((3, n)), dma((3, n)),
    ]
    taps = conv_weight.reshape(3, 2, cr).transpose(1, 0, 2)
    return pl.pallas_call(
        functools.partial(fused_kernel, dims),
        out_shape=jax.ShapeDtypeStruct((rows, width), bf16),
        in_specs=[hb, vm, hb, hb, hb, hb, hb, hb, vm, vm, sm, vm, hb, hb, hb],
        out_specs=vm,
        scratch_shapes=scratch,
        compiler_params=pltpu.CompilerParams(
            collective_id=0, has_side_effects=True, vmem_limit_bytes=56 * 1024 * 1024
        ),
    )(
        tokens, norm_gain[None, :], query_weight, key_weight, value_weight, gate_weight,
        left_weight, input_weight, query_gain[None, :],
        key_gain[None, :], sink_logit[None, :], taps, out_attention, out_conv,
        jnp.asarray(trig_table(plane * line)),
    )


def local_device(*args):
    tokens, query_weight, key_weight, gate_weight = args[0], args[2], args[3], args[5]
    fits = (
        lax.axis_size("sp") % 2 == 0
        and 8 <= lax.axis_size("sp") <= 16
        and lax.axis_size("tp") == 4
        and query_weight.shape[1] % 128 == 0
        and query_weight.shape[0] == 4 * HEAD_DIM
        and key_weight.shape[0] == HEAD_DIM
        and gate_weight.shape[0] == 256
        and tokens.shape[0] % 16 == 0
        and 8 * tokens.shape[0] % BLOCK == 0
    )
    return fused_device(*args) if fits else per_device(*args)


def solution(mesh):
    in_specs = (
        P(("sp", "tp"), None),
        P(),
        P("tp", "sp"),
        P("tp", "sp"),
        P("tp", "sp"),
        P("tp", "sp"),
        P("tp", "sp"),
        P("tp", "sp"),
        P(),
        P(),
        P("tp"),
        P(None, "tp"),
        P("tp", "sp"),
        P("tp", "sp"),
    )
    out_specs = P(("sp", "tp"), None)
    return jax.shard_map(
        local_device, mesh=mesh, in_specs=in_specs, out_specs=out_specs, check_vma=False
    )
```
